32 devices in a mesh: sp: 4 (over z), tp: 4 (over y, x), dp: 2 (over core).
Axes of the slice: x: 2, y: 2, z: 4, core: 2. Of those that a mesh axis runs over, the one named last changes fastest.
Arguments:
- latent: bfloat16 [2048, 2048], P(('dp', 'sp', 'tp')), parts along dimension 0, may hold values from -6 to 6
- context: bfloat16 [512, 2048], P(('dp', 'sp')), parts along dimension 0, may hold values from -6 to 6
- cond: bfloat16 [4096], P(('dp', 'sp')), parts along dimension 0, may hold values from -6 to 6
- context_cond: bfloat16 [2048], P('sp'), may hold values from -6 to 6
- norm_gain: float32 [2048], replicated, may hold values from 0.1 to 1.9
- mod_shift: bfloat16 [2048, 2048], P('sp', 'tp'), may hold values from -0.125 to 0.125
- mod_scale: bfloat16 [2048, 2048], P('sp', 'tp'), may hold values from -0.125 to 0.125
- mod_gate: bfloat16 [2048, 2048], P('sp', 'tp'), may hold values from -0.125 to 0.125
- w_query: bfloat16 [2048, 1024], P(None, 'tp'), may hold values from -0.125 to 0.125
- w_key: bfloat16 [2048, 1024], P(None, 'tp'), may hold values from -0.125 to 0.125
- w_value: bfloat16 [2048, 1024], P(None, 'tp'), may hold values from -0.125 to 0.125
- query_gain: float32 [64], replicated, may hold values from 1.4 to 2.2
- key_gain: float32 [64], replicated, may hold values from 0.1 to 1.9
- mix_lambda: float32 [8], P('tp'), may hold values from 0.3 to 0.8
- context_lift: float32 [8], P('tp'), may hold values from 1.5 to 2.5
- value_gain: float32 [128], replicated, may hold values from 0.1 to 1.9
- w_out: bfloat16 [1024, 2048], P('tp'), may hold values from -0.1875 to 0.1875
Outputs:
- output: bfloat16 [2048, 2048], P(('dp', 'sp', 'tp')), parts along dimension 0
The draws below stay inside these ranges and needn't reach their ends.
There are 2 independent parts, one for each index of `dp`. The reference program is written for one: setup_inputs(seed, part) draws one part's arguments, and reference() takes and returns one part's arrays. A program takes and returns all parts, laid end to end along the dimension named above; an argument that names none is the same for every part. Nothing has to cross between parts.
All inputs are finite; a program needn't handle non-finite values.
Results may differ from the reference program's by a relative error of at most 0.006.
Values may be sent and summed in bfloat16 or wider, within the bound.
A program may use at most 64 MiB of HBM per device.

```python
import jax
import jax.numpy as jnp
from jax import lax

D = 2048
HEADS = 8
HEAD_DIM = 64
VALUE_DIM = 128
GRID = 64
CTX = 256
LENGTH = 1024


def levels(key, shape, split, low, largest):
    loudness, own = 1.0, jax.random.fold_in(key, 6)
    for dim, parts in split:
        steps = jnp.exp(jax.random.uniform(jax.random.fold_in(own, dim), (parts,), jnp.float32, low / len(split), largest / len(split)))
        loudness = loudness * jnp.repeat(steps, shape[dim] // parts).reshape([-1 if axis == dim else 1 for axis in range(len(shape))])
    return loudness


def noise(stream_key, extent, width, limit, cuts=(), kind=jnp.bfloat16):
    array = jax.random.normal(stream_key, extent, jnp.float32) * width
    if len(cuts) > 0:
        array = levels(stream_key, extent, cuts, -0.22, 0.18) * array
    return jnp.clip(array, min=-limit, max=limit).astype(kind)


def setup_inputs(seed: int = 0, part: int = 0) -> dict:
    seeds = jax.random.split(jax.random.key(seed), 18)
    part_keys = jax.random.split(jax.random.fold_in(seeds[17], part), 18)
    return {
        "latent": noise(part_keys[0], (LENGTH, D), 1.0, 6.0, ((0, 16),)),
        "context": noise(part_keys[1], (CTX, D), 1.0, 6.0, ((0, 4),)),
        "cond": noise(part_keys[2], (D,), 1.0, 6.0, ((0, 4),)),
        "context_cond": noise(seeds[3], (D,), 1.0, 6.0, ((0, 4),)),
        "norm_gain": jnp.clip(1.0 + 0.18 * jax.random.normal(seeds[4], (D,), jnp.float32), 0.1, 1.9),
        "mod_shift": noise(seeds[5], (D, D), D ** -0.5, 0.125, ((0, 4), (1, 4))),
        "mod_scale": noise(seeds[6], (D, D), D ** -0.5, 0.125, ((0, 4), (1, 4))),
        "mod_gate": noise(seeds[7], (D, D), D ** -0.5, 0.125, ((0, 4), (1, 4))),
        "w_query": noise(seeds[8], (D, 2 * HEADS * HEAD_DIM), D ** -0.5, 0.125, ((1, 4),)),
        "w_key": noise(seeds[9], (D, 2 * HEADS * HEAD_DIM), D ** -0.5, 0.125, ((1, 4),)),
        "w_value": noise(seeds[10], (D, HEADS * VALUE_DIM), D ** -0.5, 0.125, ((1, 4),)),
        "query_gain": jnp.clip(jax.random.uniform(seeds[11], (HEAD_DIM,), jnp.float32, 1.4, 2.2), 1.4, 2.2),
        "key_gain": jnp.clip(1.0 + 0.18 * jax.random.normal(seeds[12], (HEAD_DIM,), jnp.float32), 0.1, 1.9),
        "mix_lambda": jnp.clip(0.3 + 0.5 * jax.random.uniform(seeds[13], (HEADS,), jnp.float32) ** levels(seeds[13], (HEADS,), ((0, 4),), -0.2, 0.2), 0.3, 0.8),
        "context_lift": jnp.clip(1.5 + 1.0 * jax.random.uniform(seeds[14], (HEADS,), jnp.float32) ** levels(seeds[14], (HEADS,), ((0, 4),), -0.2, 0.2), 1.5, 2.5),
        "value_gain": jnp.clip(1.0 + 0.18 * jax.random.normal(seeds[15], (VALUE_DIM,), jnp.float32), 0.1, 1.9),
        "w_out": noise(seeds[16], (HEADS * VALUE_DIM, D), (HEADS * VALUE_DIM) ** -0.5, 0.1875, ((0, 4),)),
    }


token_eps = 0.01
head_eps = 0.001
rope_base = 10000.0
head_factor = 0.8

def modulated_norm(row_block, gain_vector, shift_vector, scale_vector):
    values = row_block.astype(jnp.float32)
    inverse = lax.rsqrt(lax.optimization_barrier(jnp.mean(values * values, axis=-1, keepdims=True)) + token_eps)
    return (values * inverse * gain_vector * (1.0 + scale_vector) + shift_vector).astype(jnp.bfloat16)

def head_norm(values, gain_vector):
    inverse = lax.rsqrt(lax.optimization_barrier(jnp.mean(values * values, axis=-1, keepdims=True)) + token_eps)
    return values * inverse * gain_vector

def rotate(values, positions):
    quarter = values.shape[-1] // 4
    inverse = rope_base ** (-jnp.arange(quarter, dtype=jnp.float32) / quarter)
    grid_row = (positions // GRID).astype(jnp.float32)
    grid_col = (positions % GRID).astype(jnp.float32)
    angles = jnp.stack([grid_row[:, None] * inverse, grid_col[:, None] * inverse], axis=1)
    cosine_table = jnp.cos(angles)[:, None, None]
    sine_table = jnp.sin(angles)[:, None, None]
    halves = values.reshape(values.shape[:3] + (2, 2, quarter))
    front_half = halves[..., 0, :]
    back_half = halves[..., 1, :]
    turned = jnp.stack([front_half * cosine_table - back_half * sine_table, back_half * cosine_table + front_half * sine_table], axis=-2)
    return turned.reshape(values.shape)

def project_heads(row_block, weight, gain_vector, positions, factor):
    row_count = row_block.shape[0]
    head_width = gain_vector.shape[0]
    product = jnp.dot(row_block, weight, preferred_element_type=jnp.float32)
    shaped = head_norm(product.reshape(row_count, -1, 2, head_width), gain_vector)
    if positions is not None:
        shaped = rotate(shaped, positions)
    return (shaped * factor).astype(jnp.bfloat16).reshape(row_count, -1)

def attend_block(query_block, latent_keys, latent_values, context_keys, context_values, mix_lambda, context_lift, value_gain):
    head_count = mix_lambda.shape[0]
    head_width = latent_keys.shape[1] // (2 * head_count)
    shaped_query = query_block.astype(jnp.float32).reshape(query_block.shape[0], head_count, 2, head_width)

    def one_side(key_slab, value_slab, extra):
        shaped_keys = key_slab.astype(jnp.float32).reshape(key_slab.shape[0], head_count, 2, head_width)
        shaped_values = value_slab.astype(jnp.float32).reshape(value_slab.shape[0], head_count, -1)
        scores = jnp.einsum('qhmd,phmd->mhqp', shaped_query, shaped_keys) + extra
        weights = jnp.exp(scores)
        rounded = lax.optimization_barrier(weights.astype(jnp.bfloat16)).astype(jnp.float32)
        return (jnp.einsum('mhqp,phe->mhqe', rounded, shaped_values), lax.optimization_barrier(jnp.sum(weights, axis=-1)))
    latent_numer, latent_total = one_side(latent_keys, latent_values, jnp.float32(0.0))
    context_numer, context_total = one_side(context_keys, context_values, context_lift[None, :, None, None])
    ratios = (latent_numer + context_numer) / (latent_total + context_total)[..., None]
    mixed_heads = ratios[0] - mix_lambda[:, None, None] * ratios[1]
    inverse = lax.rsqrt(lax.optimization_barrier(jnp.mean(mixed_heads * mixed_heads, axis=-1, keepdims=True)) + head_eps)
    normalized = (mixed_heads * inverse * value_gain * head_factor).astype(jnp.bfloat16)
    return jnp.transpose(normalized, (1, 0, 2)).reshape(query_block.shape[0], -1)

def reference(latent, context, cond, context_cond, norm_gain, mod_shift, mod_scale, mod_gate, w_query, w_key, w_value, query_gain, key_gain, mix_lambda, context_lift, value_gain, w_out):
    cond_act = jax.nn.silu(cond.astype(jnp.float32)).astype(jnp.bfloat16)
    context_act = jax.nn.silu(context_cond.astype(jnp.float32)).astype(jnp.bfloat16)
    shift = jnp.dot(cond_act, mod_shift, preferred_element_type=jnp.float32)
    scale = jnp.dot(cond_act, mod_scale, preferred_element_type=jnp.float32)
    gate = jnp.dot(cond_act, mod_gate, preferred_element_type=jnp.float32)
    context_shift = jnp.dot(context_act, mod_shift, preferred_element_type=jnp.float32)
    context_scale = jnp.dot(context_act, mod_scale, preferred_element_type=jnp.float32)
    normed = modulated_norm(latent, norm_gain, shift, scale)
    context_normed = modulated_norm(context, norm_gain, context_shift, context_scale)
    length = latent.shape[0]
    positions = jnp.arange(length, dtype=jnp.int32)
    queries = project_heads(normed, w_query, query_gain, positions, HEAD_DIM ** (-0.5))
    latent_keys = project_heads(normed, w_key, key_gain, positions, 1.0)
    latent_values = jnp.dot(normed, w_value, preferred_element_type=jnp.float32).astype(jnp.bfloat16)
    context_keys = project_heads(context_normed, w_key, key_gain, None, 1.0)
    context_values = jnp.dot(context_normed, w_value, preferred_element_type=jnp.float32).astype(jnp.bfloat16)
    block_rows = 512 if length % 512 == 0 else length
    query_blocks = queries.reshape(length // block_rows, block_rows, -1)
    head_out = lax.map(lambda block_query: attend_block(block_query, latent_keys, latent_values, context_keys, context_values, mix_lambda, context_lift, value_gain), query_blocks).reshape(length, -1)
    mixture = jnp.dot(head_out, w_out, preferred_element_type=jnp.float32)
    return (latent.astype(jnp.float32) + gate * mixture).astype(jnp.bfloat16)
```

```python
import functools

import jax
import jax.numpy as jnp
import numpy as np
from jax import lax
from jax.experimental import pallas as pl
from jax.experimental.pallas import tpu as pltpu
from jax.sharding import PartitionSpec as P

GRID = 64
token_eps = 0.01
head_eps = 0.001
rope_base = 10000.0
head_factor = 0.8
MESH = pl.DeviceIdType.MESH
BF = jnp.bfloat16
F32 = jnp.float32


def rope_tables(length, width):
    quarter = width // 4
    inverse = (rope_base ** (-np.arange(quarter, dtype=np.float64) / quarter)).astype(np.float32)
    pos = np.arange(length)
    row = (pos // GRID).astype(np.float32)[:, None] * inverse
    col = (pos % GRID).astype(np.float32)[:, None] * inverse
    cos = np.concatenate([np.cos(row), np.cos(row), np.cos(col), np.cos(col)], axis=1)
    sin = np.concatenate([-np.sin(row), np.sin(row), -np.sin(col), np.sin(col)], axis=1)
    return np.tile(cos, (1, 2)).astype(np.float32), np.tile(sin, (1, 2)).astype(np.float32)


def kernel(n_sp, n_tp, n_dp, head_width, *refs):
    (
        lat_h, ctx_h, cond_r, cctx_r, gain_r, ms_h, msc_h, mg_h, wq_h, wk_h, wv_h,
        small_r, lam_r, lift_r, wo_h, cos_h, sin_h,
        out_r,
        lat, ctx, mw, wq, wk, wv, wo, cosv, sinv,
        act, part, mod_in, summed, mod_full, vecs, normed, qm, kv, acc, mine, ho,
        loc, bs_lat, br_lat, bs_mod, br_mod, bs_mt, br_mt, bs_kv, br_kv, bs_wo, br_wo,
        bs_dd, br_dd, bs_ho, br_ho,
    ) = refs
    s = lax.axis_index("sp")
    t = lax.axis_index("tp")
    d_ix = lax.axis_index("dp")
    core = lax.rem(d_ix, 2)
    partner = d_ix + 1 - 2 * core
    t_odd = lax.rem(t, 2)
    nbr1 = t + 1 - 2 * t_odd
    nbr2 = lax.rem(t + 2, 4)
    nbr3 = lax.rem(nbr1 + 2, 4)
    peers = (t, nbr1, nbr2, nbr3)
    R = lat.shape[1]
    HR = R // 2
    C = ctx.shape[0]
    D = lat.shape[2]
    QW = wq.shape[1]
    n_head = QW // (2 * head_width)
    HW = 2 * head_width
    VW = wv.shape[1] // n_head
    ROWS = 4 * R

    def local(i, src, dst):
        c = pltpu.make_async_copy(src, dst, loc.at[i])
        c.start()
        return c

    l_lat = local(0, lat_h, lat.at[0])
    l_mod = [local(1 + j, h, mw.at[j]) for j, h in enumerate((ms_h, msc_h, mg_h))]
    l_ctx = local(4, ctx_h, ctx)
    l_wk = local(5, wk_h, wk)
    l_wv = local(6, wv_h, wv)
    l_wq = local(7, wq_h, wq)
    l_wo = local(8, wo_h, wo.at[0])
    l_cos = local(9, cos_h.at[pl.ds(s * ROWS, ROWS)], cosv)
    l_sin = local(10, sin_h.at[pl.ds(s * ROWS, ROWS)], sinv)

    bar = pltpu.get_barrier_semaphore()
    for k in range(1, n_sp):
        pl.semaphore_signal(bar, inc=1, device_id={"sp": lax.rem(s + k, n_sp)}, device_id_type=MESH)
    for k in range(1, 4):
        pl.semaphore_signal(bar, inc=1, device_id={"tp": peers[k]}, device_id_type=MESH)
    pl.semaphore_signal(bar, inc=1, device_id={"dp": partner}, device_id_type=MESH)

    act[...] = jnp.zeros_like(act)
    for row, ref in ((0, cond_r), (1, cctx_r)):
        v = ref[...].astype(F32)
        act[row : row + 1, :] = v / (1.0 + jnp.exp(-v))
    acts = act[...].astype(BF)
    part[...] = jnp.zeros_like(part)
    for j in range(3):
        l_mod[j].wait()
        res = jnp.dot(acts, mw[j], preferred_element_type=F32)
        part[2 * j : 2 * j + 2, :] = res[0:2]

    pl.semaphore_wait(bar, n_sp + 3)

    def remote(src, dst, ss, rs, where):
        return pltpu.make_async_remote_copy(
            src_ref=src, dst_ref=dst, send_sem=ss, recv_sem=rs, device_id=where, device_id_type=MESH
        )

    mod_copies = []
    for k in range(1, n_sp):
        c = remote(part, mod_in.at[k - 1], bs_mod.at[k - 1], br_mod.at[k - 1],
                   {"sp": lax.rem(s + k, n_sp)})
        c.start()
        mod_copies.append(c)

    l_lat.wait()

    def lat_copy(i, src_slot, dst_slot, half, where):
        rows = pl.ds(half * HR, HR)
        return remote(lat.at[src_slot, rows], lat.at[dst_slot, rows], bs_lat.at[i], br_lat.at[i],
                      {"tp": where})

    x0 = lat_copy(0, 0, 1, 0, nbr1)
    y1 = lat_copy(1, 0, 2, 1, nbr2)
    x1 = lat_copy(2, 0, 1, 1, nbr1)
    y0 = lat_copy(3, 0, 2, 0, nbr2)
    f0 = lat_copy(4, 1, 3, 0, nbr2)
    f1 = lat_copy(5, 2, 3, 1, nbr1)
    for c in (x0, y1, x1, y0):
        c.start()

    total = part[...]
    for k in range(n_sp - 1):
        mod_copies[k].wait_recv()
        total = total + mod_in[k]
    summed[...] = total
    mod_full[t] = total
    tp_copies = []
    for k in range(1, 4):
        c = remote(summed, mod_full.at[t], bs_mt.at[k - 1], br_mt.at[k - 1], {"tp": peers[k]})
        c.start()
        tp_copies.append(c)
    x0.wait_recv()
    f0.start()
    y1.wait_recv()
    f1.start()

    for k in range(1, 4):
        remote(summed, mod_full.at[peers[k]], bs_mt.at[k - 1], br_mt.at[k - 1],
               {"tp": peers[k]}).wait_recv()

    def full_row(j):
        return jnp.concatenate([mod_full[q, j : j + 1, :] for q in range(n_tp)], axis=1)

    gain = gain_r[...]
    vecs[0:1, :] = full_row(0)
    vecs[1:2, :] = full_row(1)
    vecs[2:3, :] = gain * (1.0 + full_row(2))
    vecs[3:4, :] = gain * (1.0 + full_row(3))
    vecs[4:5, :] = full_row(4)

    HALF = wo.shape[1] // 2
    QUART = HALF // 2

    def wo_rows(q):
        return pl.ds(pl.multiple_of(core * HALF + q * QUART, QUART), QUART)

    def wo_copy(i, src_slot, dst_slot, q, where):
        return remote(wo.at[src_slot, wo_rows(q)], wo.at[dst_slot, wo_rows(q)], bs_wo.at[i],
                      br_wo.at[i], {"tp": where})

    def dd_copy(k):
        rows = pl.ds(pl.multiple_of(core * HALF, HALF), HALF)
        return remote(wo.at[k, rows], wo.at[k, rows], bs_dd.at[k - 1], br_dd.at[k - 1],
                      {"dp": partner})

    def dd_recv(k):
        rows = pl.ds(pl.multiple_of((1 - core) * HALF, HALF), HALF)
        return remote(wo.at[k, rows], wo.at[k, rows], bs_dd.at[k - 1], br_dd.at[k - 1],
                      {"dp": partner})

    wx0 = wo_copy(0, 0, 1, 0, nbr1)
    wy1 = wo_copy(1, 0, 2, 1, nbr2)
    wx1 = wo_copy(2, 0, 1, 1, nbr1)
    wy0 = wo_copy(3, 0, 2, 0, nbr2)
    wf0 = wo_copy(4, 1, 3, 0, nbr2)
    wf1 = wo_copy(5, 2, 3, 1, nbr1)

    def norm_rows(src, row, count, dst_at):
        step = 16

        @pl.loop(0, count // step)
        def _(i):
            at = pl.multiple_of(i * step, step)
            v = src[pl.ds(at, step), :].astype(F32)
            inv = lax.rsqrt(jnp.mean(v * v, axis=-1, keepdims=True) + token_eps)
            normed[pl.ds(dst_at + at, step), :] = (
                v * inv * vecs[2 + row : 3 + row, :] + vecs[row : row + 1, :]
            ).astype(BF)

    group = (
        lax.broadcasted_iota(jnp.int32, (QW, QW), 0) // head_width
        == lax.broadcasted_iota(jnp.int32, (QW, QW), 1) // head_width
    )
    group = jnp.where(group, 1.0 / head_width, 0.0).astype(F32)

    def head_norm(x):
        mean = jnp.dot(x * x, group, precision=lax.Precision.HIGHEST, preferred_element_type=F32)
        return x * lax.rsqrt(mean + token_eps)

    def turn(y, cos, sin):
        lane = lax.broadcasted_iota(jnp.int32, y.shape, 1)
        front = lax.rem(lane, head_width // 2) < head_width // 4
        other = jnp.where(
            front,
            pltpu.roll(y, HW - head_width // 4, axis=1),
            pltpu.roll(y, head_width // 4, axis=1),
        )
        return y * cos + other * sin

    def project_block(k, first):
        rows = pl.ds(first + C, R)
        x = normed[C + k * R : C + (k + 1) * R, :]
        at = pl.ds(pl.multiple_of(peers[k] * R, R), R)
        cos, sin = cosv[at, :], sinv[at, :]
        kk = head_norm(jnp.dot(x, wk[...], preferred_element_type=F32))
        for h in range(n_head):
            y = kk[:, h * HW : (h + 1) * HW] * small_r[1:2, :HW]
            kv[s, rows, h * HW : (h + 1) * HW] = turn(y, cos, sin).astype(BF)
        kv[s, rows, QW:] = jnp.dot(x, wv[...], preferred_element_type=F32).astype(BF)

    def project_queries():
        x = normed[C:, :]
        qq = head_norm(jnp.dot(x, wq[...], preferred_element_type=F32))
        for k in range(4):
            at = pl.ds(pl.multiple_of(peers[k] * R, R), R)
            cos, sin = cosv[at, :], sinv[at, :]
            for h in range(n_head):
                y = qq[k * R : (k + 1) * R, h * HW : (h + 1) * HW] * small_r[0:1, :HW]
                y = turn(y, cos, sin) * (head_width ** -0.5)
                lane = lax.broadcasted_iota(jnp.int32, y.shape, 1)
                for m in range(2):
                    keep = (lane // head_width) == m
                    qm[2 * h + m, k * R : (k + 1) * R, :] = jnp.where(keep, y, 0.0).astype(BF)

    chunks = ((0, C + R), (C + R, 2 * R), (C + 3 * R, R))

    def kv_copy(direction, dist, c, origin, where):
        at, count = chunks[c]
        piece = kv.at[origin, pl.ds(at, count)]
        i = (direction * (n_sp - 1) + dist - 1) * len(chunks) + c
        return remote(piece, piece, bs_kv.at[i], br_kv.at[i], {"sp": where})

    def right_to(dist, c):
        return kv_copy(0, dist, c, s - (dist - 1), s + 1)

    def left_to(dist, c):
        return kv_copy(1, dist, c, s + (dist - 1), s - 1)

    def send_own(c):
        @pl.when(s + 1 < n_sp)
        def _():
            right_to(1, c).start()

        @pl.when(s >= 1)
        def _():
            left_to(1, c).start()

    l_ctx.wait()
    norm_rows(ctx, 1, C, 0)
    norm_rows(lat.at[0], 0, R, C)
    l_wk.wait()
    l_wv.wait()
    l_cos.wait()
    l_sin.wait()
    x = normed[0:C, :]
    kk = head_norm(jnp.dot(x, wk[...], preferred_element_type=F32))
    for h in range(n_head):
        kv[s, 0:C, h * HW : (h + 1) * HW] = (
            kk[:, h * HW : (h + 1) * HW] * small_r[1:2, :HW]
        ).astype(BF)
    kv[s, 0:C, QW:] = jnp.dot(x, wv[...], preferred_element_type=F32).astype(BF)
    project_block(0, 0)
    send_own(0)

    x1.wait_recv()
    y0.wait_recv()
    l_wo.wait()
    for c in (wx0, wy1, wx1, wy0):
        c.start()
    norm_rows(lat.at[1], 0, R, C + R)
    norm_rows(lat.at[2], 0, R, C + 2 * R)
    project_block(1, R)
    project_block(2, 2 * R)
    send_own(1)
    f0.wait_recv()
    f1.wait_recv()
    norm_rows(lat.at[3], 0, R, C + 3 * R)
    project_block(3, 3 * R)
    send_own(2)
    l_wq.wait()
    project_queries()

    QB = 2 * R

    def attend(slot, first):
        keys = C + ROWS
        is_ctx = lax.broadcasted_iota(jnp.int32, (1, keys), 1) < C
        for h in range(n_head):
            k = kv[slot, :, h * HW : (h + 1) * HW]
            v = kv[slot, :, QW + h * VW : QW + (h + 1) * VW]
            vx = jnp.concatenate([v, jnp.ones_like(v)], axis=1)
            bias = jnp.where(is_ctx, lift_r[h], 0.0)
            for m in range(2):
                for b in range(ROWS // QB):
                    rows = slice(b * QB, (b + 1) * QB)
                    sc = lax.dot_general(
                        qm[2 * h + m, rows, :], k, (((1,), (1,)), ((), ())),
                        preferred_element_type=F32,
                    )
                    p = jnp.exp(sc + bias).astype(BF)
                    add = jnp.dot(p, vx, preferred_element_type=F32)
                    if first:
                        acc[2 * h + m, rows, :] = add
                    else:
                        acc[2 * h + m, rows, :] += add

    attend(s, True)

    for dist in range(1, n_sp):
        for c in range(len(chunks)):
            @pl.when(s - dist >= 0)
            def _():
                kv_copy(0, dist, c, s - dist, s).wait_recv()

            if dist < n_sp - 1:
                @pl.when(jnp.logical_and(s - dist >= 0, s + 1 < n_sp))
                def _():
                    right_to(dist + 1, c).start()

            @pl.when(s + dist < n_sp)
            def _():
                kv_copy(1, dist, c, s + dist, s).wait_recv()

            if dist < n_sp - 1:
                @pl.when(jnp.logical_and(s + dist < n_sp, s >= 1))
                def _():
                    left_to(dist + 1, c).start()

        if dist == 1:
            wx0.wait_recv()
            wf0.start()
            wy1.wait_recv()
            wf1.start()
        if dist == 2:
            wx1.wait_recv()
            dd_copy(1).start()
            wy0.wait_recv()
            dd_copy(2).start()
        if dist == n_sp - 1:
            wf0.wait_recv()
            wf1.wait_recv()
            dd_copy(3).start()

        @pl.when(s - dist >= 0)
        def _():
            attend(s - dist, False)

        @pl.when(s + dist < n_sp)
        def _():
            attend(s + dist, False)

    def ho_copy(k):
        return remote(mine.at[k], ho.at[k], bs_ho.at[k], br_ho.at[k], {"tp": peers[k]})

    for k in (3, 1, 2, 0):
        rows = slice(k * R, (k + 1) * R)
        for h in range(n_head):
            a0 = acc[2 * h, rows, :]
            a1 = acc[2 * h + 1, rows, :]
            mixed = a0[:, :VW] / a0[:, VW:] - lam_r[h] * (a1[:, :VW] / a1[:, VW:])
            inv = lax.rsqrt(jnp.mean(mixed * mixed, axis=-1, keepdims=True) + head_eps)
            mine[k, :, h * VW : (h + 1) * VW] = (
                mixed * inv * small_r[2:3, :VW] * head_factor
            ).astype(BF)
        if k:
            ho_copy(k).start()

    for k in range(1, 4):
        dd_recv(k).wait_recv()
    out = jnp.dot(mine[0], wo[0], preferred_element_type=F32)
    for k in (1, 2, 3):
        ho_copy(k).wait_recv()
        out += jnp.dot(ho[k], wo[k], preferred_element_type=F32)
    out_r[...] = (lat[0].astype(F32) + vecs[4:5, :] * out).astype(BF)

    for c in mod_copies + tp_copies + [x0, y1, x1, y0, f0, f1, wx0, wy1, wx1, wy0, wf0, wf1]:
        c.wait_send()
    for k in range(1, 4):
        dd_copy(k).wait_send()
        ho_copy(k).wait_send()
    for dist in range(1, n_sp):
        for c in range(len(chunks)):
            @pl.when(jnp.logical_and(s - (dist - 1) >= 0, s + 1 < n_sp))
            def _():
                right_to(dist, c).wait_send()

            @pl.when(jnp.logical_and(s + (dist - 1) < n_sp, s >= 1))
            def _():
                left_to(dist, c).wait_send()


def on_device(n_sp, n_tp, n_dp, *args):
    (
        latent, context, cond, context_cond, norm_gain, mod_shift, mod_scale, mod_gate,
        w_query, w_key, w_value, query_gain, key_gain, mix_lambda, context_lift, value_gain, w_out,
    ) = args
    R, D = latent.shape
    C = context.shape[0]
    head_width = query_gain.shape[0]
    cos, sin = rope_tables(R * n_sp * n_tp, head_width)
    small = jnp.stack([jnp.tile(query_gain, 2), jnp.tile(key_gain, 2), value_gain])
    QW, VWALL = w_query.shape[1], w_value.shape[1]
    heads = mix_lambda.shape[0]
    ROWS = R * n_tp
    MC = mod_shift.shape[1]
    chunk_sems = 2 * max(n_sp - 1, 1) * 3
    vm = pl.BlockSpec(memory_space=pltpu.VMEM)
    anywhere = pl.BlockSpec(memory_space=pl.ANY)
    smem = pl.BlockSpec(memory_space=pltpu.SMEM)
    dma = pltpu.SemaphoreType.DMA
    return pl.pallas_call(
        functools.partial(kernel, n_sp, n_tp, n_dp, head_width),
        out_shape=jax.ShapeDtypeStruct((R, D), latent.dtype),
        in_specs=[anywhere, anywhere, vm, vm, vm] + [anywhere] * 6 + [vm, smem, smem]
        + [anywhere] * 3,
        out_specs=vm,
        scratch_shapes=[
            pltpu.VMEM((4, R, D), BF),
            pltpu.VMEM((C, D), BF),
            pltpu.VMEM((3,) + mod_shift.shape, BF),
            pltpu.VMEM(w_query.shape, BF),
            pltpu.VMEM(w_key.shape, BF),
            pltpu.VMEM(w_value.shape, BF),
            pltpu.VMEM((4,) + w_out.shape, BF),
            pltpu.VMEM((ROWS, 2 * head_width), F32),
            pltpu.VMEM((ROWS, 2 * head_width), F32),
            pltpu.VMEM((8, mod_shift.shape[0]), F32),
            pltpu.VMEM((8, MC), F32),
            pltpu.VMEM((max(n_sp - 1, 1), 8, MC), F32),
            pltpu.VMEM((8, MC), F32),
            pltpu.VMEM((n_tp, 8, MC), F32),
            pltpu.VMEM((8, D), F32),
            pltpu.VMEM((C + ROWS, D), BF),
            pltpu.VMEM((2 * heads, ROWS, 2 * head_width), BF),
            pltpu.VMEM((n_sp, C + ROWS, QW + VWALL), BF),
            pltpu.VMEM((2 * heads, ROWS, 2 * VWALL // heads), F32),
            pltpu.VMEM((4, R, VWALL), BF),
            pltpu.VMEM((4, R, VWALL), BF),
            dma((11,)),
            dma((6,)), dma((6,)),
            dma((max(n_sp - 1, 1),)), dma((max(n_sp - 1, 1),)),
            dma((3,)), dma((3,)),
            dma((chunk_sems,)), dma((chunk_sems,)),
            dma((6,)), dma((6,)),
            dma((3,)), dma((3,)),
            dma((4,)), dma((4,)),
        ],
        compiler_params=pltpu.CompilerParams(
            collective_id=0, has_side_effects=True, vmem_limit_bytes=60 * 1024 * 1024
        ),
        name="block",
    )(
        latent, context, cond[None], context_cond[None], norm_gain[None], mod_shift, mod_scale,
        mod_gate, w_query, w_key, w_value, small, mix_lambda, context_lift, w_out,
        jnp.asarray(cos), jnp.asarray(sin),
    )


def solution(mesh):
    placed = (
        P(("dp", "sp", "tp"), None),
        P(("dp", "sp"), None),
        P(("dp", "sp")),
        P("sp"),
        P(),
        P("sp", "tp"),
        P("sp", "tp"),
        P("sp", "tp"),
        P(None, "tp"),
        P(None, "tp"),
        P(None, "tp"),
        P(),
        P(),
        P("tp"),
        P("tp"),
        P(),
        P("tp", None),
    )
    sizes = mesh.shape
    return jax.shard_map(
        functools.partial(on_device, sizes["sp"], sizes["tp"], sizes["dp"]),
        mesh=mesh,
        in_specs=placed,
        out_specs=P(("dp", "sp", "tp"), None),
        check_vma=False,
    )
```

```python
import functools

import jax
import jax.numpy as jnp
import numpy as np
from jax import lax
from jax.experimental import pallas as pl
from jax.experimental.pallas import tpu as pltpu
from jax.sharding import PartitionSpec as P

GRID = 64
token_eps = 0.01
head_eps = 0.001
rope_base = 10000.0
head_factor = 0.8
MESH = pl.DeviceIdType.MESH
BF = jnp.bfloat16
F32 = jnp.float32


def rope_tables(length, width):
    quarter = width // 4
    inverse = (rope_base ** (-np.arange(quarter, dtype=np.float64) / quarter)).astype(np.float32)
    pos = np.arange(length)
    row = (pos // GRID).astype(np.float32)[:, None] * inverse
    col = (pos % GRID).astype(np.float32)[:, None] * inverse
    cos = np.concatenate([np.cos(row), np.cos(row), np.cos(col), np.cos(col)], axis=1)
    sin = np.concatenate([-np.sin(row), np.sin(row), -np.sin(col), np.sin(col)], axis=1)
    return np.tile(cos, (1, 2)).astype(np.float32), np.tile(sin, (1, 2)).astype(np.float32)


def kernel(n_sp, n_tp, n_dp, head_width, *refs):
    (
        lat_h, ctx_h, cond_h, cctx_h, gain_h, ms_h, msc_h, mg_h, wq_h, wk_h, wv_h,
        qg_h, kg_h, vg_h, lam_r, lift_r, wo_h, cos_h, sin_h,
        out_r,
        cond_r, cctx_r, gain_r, qg_r, kg_r, vg_r,
        lat, ctx, mw, wq, wk, wv, wo, cosv, sinv,
        act, part, mod_in, summed, mod_full, vecs, normed, qown, qin, qm, kvl, kvr, acc, mine, ho,
        loc, bs_lat, br_lat, bs_mod, br_mod, bs_mt, br_mt, bs_kv, br_kv, bs_wo, br_wo,
        bs_dd, br_dd, bs_ho, br_ho, bs_q, br_q,
    ) = refs
    s = lax.axis_index("sp")
    t = lax.axis_index("tp")
    d_ix = lax.axis_index("dp")
    core = lax.rem(d_ix, 2)
    partner = d_ix + 1 - 2 * core
    t_odd = lax.rem(t, 2)
    nbr1 = t + 1 - 2 * t_odd
    nbr2 = lax.rem(t + 2, 4)
    nbr3 = lax.rem(nbr1 + 2, 4)
    peers = (t, nbr1, nbr2, nbr3)
    e = lax.rem(s, 2)
    pair = s + 1 - 2 * e
    R = lat.shape[1]
    HR = R // 2
    C = ctx.shape[0]
    D = lat.shape[2]
    QW = wq.shape[1]
    n_head = QW // (2 * head_width)
    HW = 2 * head_width
    VW = wv.shape[1] // n_head
    ROWS = 4 * R

    def local(i, src, dst):
        c = pltpu.make_async_copy(src, dst, loc.at[i])
        c.start()
        return c

    l_one = [
        local(11 + j, src, dst)
        for j, (src, dst) in enumerate(
            ((cond_h, cond_r), (cctx_h, cctx_r), (gain_h, gain_r), (qg_h, qg_r), (kg_h, kg_r),
             (vg_h, vg_r))
        )
    ]
    l_lat = local(0, lat_h, lat.at[0])
    l_mod = [local(1 + j, h, mw.at[j]) for j, h in enumerate((ms_h, msc_h, mg_h))]
    l_ctx = local(4, ctx_h, ctx)
    l_wk = local(5, wk_h, wk)
    l_wv = local(6, wv_h, wv)
    l_wq = local(7, wq_h, wq)
    l_wo = local(8, wo_h, wo.at[0])
    l_cos = local(9, cos_h.at[pl.ds(s * ROWS, ROWS)], cosv)
    l_sin = local(10, sin_h.at[pl.ds(s * ROWS, ROWS)], sinv)

    bar = pltpu.get_barrier_semaphore()
    for k in range(1, n_sp):
        pl.semaphore_signal(bar, inc=1, device_id={"sp": lax.rem(s + k, n_sp)}, device_id_type=MESH)
    for k in range(1, 4):
        pl.semaphore_signal(bar, inc=1, device_id={"tp": peers[k]}, device_id_type=MESH)
        pl.semaphore_signal(
            bar, inc=1, device_id={"sp": pair, "tp": peers[k]}, device_id_type=MESH
        )
    pl.semaphore_signal(bar, inc=1, device_id={"dp": partner}, device_id_type=MESH)

    act[...] = jnp.zeros_like(act)
    for row, ref in ((0, cond_r), (1, cctx_r)):
        l_one[row].wait()
        v = ref[...].astype(F32).reshape(1, -1)
        act[row : row + 1, :] = v / (1.0 + jnp.exp(-v))
    acts = act[...].astype(BF)
    part[...] = jnp.zeros_like(part)
    for j in range(3):
        l_mod[j].wait()
        res = jnp.dot(acts, mw[j], preferred_element_type=F32)
        part[2 * j : 2 * j + 2, :] = res[0:2]

    pl.semaphore_wait(bar, n_sp + 6)

    def remote(src, dst, ss, rs, where):
        return pltpu.make_async_remote_copy(
            src_ref=src, dst_ref=dst, send_sem=ss, recv_sem=rs, device_id=where, device_id_type=MESH
        )

    mod_copies = []
    for k in range(1, n_sp):
        c = remote(part, mod_in.at[k - 1], bs_mod.at[k - 1], br_mod.at[k - 1],
                   {"sp": lax.rem(s + k, n_sp)})
        c.start()
        mod_copies.append(c)

    l_lat.wait()

    def lat_copy(i, src_slot, dst_slot, half, where):
        rows = pl.ds(half * HR, HR)
        return remote(lat.at[src_slot, rows], lat.at[dst_slot, rows], bs_lat.at[i], br_lat.at[i],
                      {"tp": where})

    x0 = lat_copy(0, 0, 1, 0, nbr1)
    y1 = lat_copy(1, 0, 2, 1, nbr2)
    x1 = lat_copy(2, 0, 1, 1, nbr1)
    y0 = lat_copy(3, 0, 2, 0, nbr2)
    f0 = lat_copy(4, 1, 3, 0, nbr2)
    f1 = lat_copy(5, 2, 3, 1, nbr1)
    for c in (x0, y1):
        c.start()

    total = part[...]
    for k in range(n_sp - 1):
        mod_copies[k].wait_recv()
        total = total + mod_in[k]
    summed[...] = total
    mod_full[t] = total
    tp_copies = []
    for k in range(1, 4):
        c = remote(summed, mod_full.at[t], bs_mt.at[k - 1], br_mt.at[k - 1], {"tp": peers[k]})
        c.start()
        tp_copies.append(c)
    x1.start()
    y0.start()
    x0.wait_recv()
    f0.start()
    y1.wait_recv()
    f1.start()

    for k in range(1, 4):
        remote(summed, mod_full.at[peers[k]], bs_mt.at[k - 1], br_mt.at[k - 1],
               {"tp": peers[k]}).wait_recv()

    def full_row(j):
        return jnp.concatenate([mod_full[q, j : j + 1, :] for q in range(n_tp)], axis=1)

    for c in l_one[2:]:
        c.wait()
    gain = gain_r[...].reshape(1, -1)
    q_gain = qg_r[...].reshape(1, -1)
    q_gain = jnp.concatenate([q_gain, q_gain], axis=1)
    k_gain = kg_r[...].reshape(1, -1)
    k_gain = jnp.concatenate([k_gain, k_gain], axis=1)
    v_gain = vg_r[...].reshape(1, -1)
    vecs[0:1, :] = full_row(0)
    vecs[1:2, :] = full_row(1)
    vecs[2:3, :] = gain * (1.0 + full_row(2))
    vecs[3:4, :] = gain * (1.0 + full_row(3))
    vecs[4:5, :] = full_row(4)

    HALF = wo.shape[1] // 2
    QUART = HALF // 2

    def wo_rows(q):
        return pl.ds(pl.multiple_of(core * HALF + q * QUART, QUART), QUART)

    def wo_copy(i, src_slot, dst_slot, q, where):
        return remote(wo.at[src_slot, wo_rows(q)], wo.at[dst_slot, wo_rows(q)], bs_wo.at[i],
                      br_wo.at[i], {"tp": where})

    def dd_copy(k):
        rows = pl.ds(pl.multiple_of(core * HALF, HALF), HALF)
        return remote(wo.at[k, rows], wo.at[k, rows], bs_dd.at[k - 1], br_dd.at[k - 1],
                      {"dp": partner})

    def dd_recv(k):
        rows = pl.ds(pl.multiple_of((1 - core) * HALF, HALF), HALF)
        return remote(wo.at[k, rows], wo.at[k, rows], bs_dd.at[k - 1], br_dd.at[k - 1],
                      {"dp": partner})

    wx0 = wo_copy(0, 0, 1, 0, nbr1)
    wy1 = wo_copy(1, 0, 2, 1, nbr2)
    wx1 = wo_copy(2, 0, 1, 1, nbr1)
    wy0 = wo_copy(3, 0, 2, 0, nbr2)
    wf0 = wo_copy(4, 1, 3, 0, nbr2)
    wf1 = wo_copy(5, 2, 3, 1, nbr1)

    def norm_rows(src, row, count, dst_at):
        step = 16

        @pl.loop(0, count // step)
        def _(i):
            at = pl.multiple_of(i * step, step)
            v = src[pl.ds(at, step), :].astype(F32)
            inv = lax.rsqrt(jnp.mean(v * v, axis=-1, keepdims=True) + token_eps)
            normed[pl.ds(dst_at + at, step), :] = (
                v * inv * vecs[2 + row : 3 + row, :] + vecs[row : row + 1, :]
            ).astype(BF)

    group = (
        lax.broadcasted_iota(jnp.int32, (QW, QW), 0) // head_width
        == lax.broadcasted_iota(jnp.int32, (QW, QW), 1) // head_width
    )
    group = jnp.where(group, 1.0 / head_width, 0.0).astype(F32)

    def head_norm(x):
        mean = jnp.dot(x * x, group, precision=lax.Precision.HIGHEST, preferred_element_type=F32)
        return x * lax.rsqrt(mean + token_eps)

    def turn(y, cos, sin):
        lane = lax.broadcasted_iota(jnp.int32, y.shape, 1)
        front = lax.rem(lane, head_width // 2) < head_width // 4
        other = jnp.where(
            front,
            pltpu.roll(y, HW - head_width // 4, axis=1),
            pltpu.roll(y, head_width // 4, axis=1),
        )
        return y * cos + other * sin

    def project_block(k, first):
        rows = pl.ds(first + C, R)
        x = normed[C + k * R : C + (k + 1) * R, :]
        at = pl.ds(pl.multiple_of(peers[k] * R, R), R)
        cos, sin = cosv[at, :], sinv[at, :]
        kk = head_norm(jnp.dot(x, wk[...], preferred_element_type=F32))
        for h in range(n_head):
            y = kk[:, h * HW : (h + 1) * HW] * k_gain
            kvl[h, rows, 0:HW] = turn(y, cos, sin).astype(BF)
        vv = jnp.dot(x, wv[...], preferred_element_type=F32).astype(BF)
        for h in range(n_head):
            kvl[h, rows, HW:] = vv[:, h * VW : (h + 1) * VW]

    def project_queries():
        x = normed[C:, :]
        qq = head_norm(jnp.dot(x, wq[...], preferred_element_type=F32))
        for k in range(4):
            at = pl.ds(pl.multiple_of(peers[k] * R, R), R)
            cos, sin = cosv[at, :], sinv[at, :]
            for h in range(n_head):
                y = qq[k * R : (k + 1) * R, h * HW : (h + 1) * HW] * q_gain
                qown[h, k * R : (k + 1) * R, :] = (
                    turn(y, cos, sin) * (head_width ** -0.5)
                ).astype(BF)

    def split_maps(q, at):
        lane = lax.broadcasted_iota(jnp.int32, q.shape, 1)
        for m in range(2):
            qm[m, at : at + ROWS, :] = jnp.where(lane // head_width == m, q, jnp.zeros_like(q))

    chunks = ((0, C + R), (C + R, 2 * R), (C + 3 * R, R))

    def kv_copy(direction, dist, c, src, origin, where):
        at, count = chunks[c]
        i = (direction * (n_sp - 1) + dist - 1) * len(chunks) + c
        return remote(src.at[pl.ds(at, count)], kvr.at[origin, pl.ds(at, count)], bs_kv.at[i],
                      br_kv.at[i], {"sp": where})

    def side(direction, dist, c, act_on):
        sign = 1 - 2 * direction
        hop = 1 if dist == 1 else 2
        origin = s - sign * (dist - hop)
        where = s + sign * hop
        ok = jnp.logical_and(
            jnp.logical_and(origin >= 0, origin < n_sp),
            jnp.logical_and(where >= 0, where < n_sp),
        )

        @pl.when(ok)
        def _():
            if dist == 1:
                src = kvl.at[1 - e]
            elif dist == 2:
                src = kvl.at[e]
            else:
                src = kvr.at[origin]
            act_on(kv_copy(direction, dist, c, src, origin, where))

    def start(copy):
        copy.start()

    def drain(copy):
        copy.wait_send()

    def send_own(c):
        for dist in (1, 2):
            if dist < n_sp:
                for direction in (0, 1):
                    side(direction, dist, c, start)

    l_ctx.wait()
    norm_rows(ctx, 1, C, 0)
    norm_rows(lat.at[0], 0, R, C)
    l_wk.wait()
    l_wv.wait()
    l_cos.wait()
    l_sin.wait()
    x = normed[0:C, :]
    kk = head_norm(jnp.dot(x, wk[...], preferred_element_type=F32))
    vv = jnp.dot(x, wv[...], preferred_element_type=F32).astype(BF)
    for h in range(n_head):
        kvl[h, 0:C, 0:HW] = (kk[:, h * HW : (h + 1) * HW] * k_gain).astype(BF)
        kvl[h, 0:C, HW:] = vv[:, h * VW : (h + 1) * VW]
    project_block(0, 0)
    send_own(0)

    x1.wait_recv()
    y0.wait_recv()
    l_wo.wait()
    for c in (wx0, wy1, wx1, wy0):
        c.start()
    norm_rows(lat.at[1], 0, R, C + R)
    norm_rows(lat.at[2], 0, R, C + 2 * R)
    project_block(1, R)
    project_block(2, 2 * R)
    send_own(1)
    f0.wait_recv()
    f1.wait_recv()
    norm_rows(lat.at[3], 0, R, C + 3 * R)
    project_block(3, 3 * R)
    send_own(2)
    l_wq.wait()
    project_queries()

    q_copy = remote(qown.at[1 - e], qin, bs_q, br_q, {"sp": pair})
    q_copy.start()
    split_maps(qown[e], 0)

    QB = 2 * R
    keys = C + ROWS
    is_ctx = lax.broadcasted_iota(jnp.int32, (1, keys), 1) < C
    bias = jnp.where(is_ctx, lift_r[e], 0.0)

    def attend(block, start_row, count, first):
        k = block[:, 0:HW]
        v = block[:, HW:]
        vx = jnp.concatenate([v, jnp.ones_like(v)], axis=1)
        for m in range(2):
            for b in range(count // QB):
                rows = slice(start_row + b * QB, start_row + (b + 1) * QB)
                sc = lax.dot_general(
                    qm[m, rows, :], k, (((1,), (1,)), ((), ())), preferred_element_type=F32
                )
                p = jnp.exp(sc + bias).astype(BF)
                add = jnp.dot(p, vx, preferred_element_type=F32)
                if first:
                    acc[m, rows, :] = add
                else:
                    acc[m, rows, :] += add

    attend(kvl.at[e], 0, ROWS, True)
    q_copy.wait_recv()
    split_maps(qin[...], ROWS)
    attend(kvl.at[e], ROWS, ROWS, True)

    for dist in range(1, n_sp):
        for c in range(len(chunks)):
            for direction in (0, 1):
                origin = s - dist if direction == 0 else s + dist
                here = origin >= 0 if direction == 0 else origin < n_sp

                @pl.when(here)
                def _():
                    kv_copy(direction, dist, c, kvr.at[origin], origin, s).wait_recv()

                if dist + 2 < n_sp:
                    side(direction, dist + 2, c, start)

        if dist == 1:
            wx0.wait_recv()
            wf0.start()
            wy1.wait_recv()
            wf1.start()
        if dist == 2:
            wx1.wait_recv()
            dd_copy(1).start()
            wy0.wait_recv()
            dd_copy(2).start()
        if dist == n_sp - 1:
            wf0.wait_recv()
            wf1.wait_recv()
            dd_copy(3).start()

        @pl.when(s - dist >= 0)
        def _():
            attend(kvr.at[s - dist], 0, 2 * ROWS, False)

        @pl.when(s + dist < n_sp)
        def _():
            attend(kvr.at[s + dist], 0, 2 * ROWS, False)

    def ho_copy(q, k):
        i = q * 4 + k
        where = {"tp": peers[k]} if q == 0 else {"sp": pair, "tp": peers[k]}
        if q == 1 and k == 0:
            where = {"sp": pair}
        return remote(mine.at[q, k], ho.at[q, k], bs_ho.at[i], br_ho.at[i], where)

    for q, k in ((1, 3), (1, 1), (1, 2), (0, 3), (1, 0), (0, 1), (0, 2), (0, 0)):
        rows = slice((4 * q + k) * R, (4 * q + k + 1) * R)
        a0 = acc[0, rows, :]
        a1 = acc[1, rows, :]
        mixed = a0[:, :VW] / a0[:, VW:] - lam_r[e] * (a1[:, :VW] / a1[:, VW:])
        inv = lax.rsqrt(jnp.mean(mixed * mixed, axis=-1, keepdims=True) + head_eps)
        mine[q, k, :, :] = (mixed * inv * v_gain * head_factor).astype(BF)
        if q or k:
            ho_copy(q, k).start()

    for k in range(1, 4):
        dd_recv(k).wait_recv()

    def head_rows(q):
        return pl.ds(pl.multiple_of((e if q == 0 else 1 - e) * VW, VW), VW)

    out = jnp.dot(mine[0, 0], wo[0, head_rows(0), :], preferred_element_type=F32)
    for q, k in ((0, 1), (0, 2), (1, 0), (0, 3), (1, 1), (1, 2), (1, 3)):
        ho_copy(q, k).wait_recv()
        out += jnp.dot(ho[q, k], wo[k, head_rows(q), :], preferred_element_type=F32)
    out_r[...] = (lat[0].astype(F32) + vecs[4:5, :] * out).astype(BF)

    for c in mod_copies + tp_copies + [x0, y1, x1, y0, f0, f1, wx0, wy1, wx1, wy0, wf0, wf1]:
        c.wait_send()
    for k in range(1, 4):
        dd_copy(k).wait_send()
    q_copy.wait_send()
    for q in range(2):
        for k in range(4):
            if q or k:
                ho_copy(q, k).wait_send()
    for dist in range(1, n_sp):
        for c in range(len(chunks)):
            for direction in (0, 1):
                side(direction, dist, c, drain)


def on_device(n_sp, n_tp, n_dp, *args):
    (
        latent, context, cond, context_cond, norm_gain, mod_shift, mod_scale, mod_gate,
        w_query, w_key, w_value, query_gain, key_gain, mix_lambda, context_lift, value_gain, w_out,
    ) = args
    R, D = latent.shape
    C = context.shape[0]
    head_width = query_gain.shape[0]
    cos, sin = rope_tables(R * n_sp * n_tp, head_width)
    QW, VWALL = w_query.shape[1], w_value.shape[1]
    heads = mix_lambda.shape[0]
    ROWS = R * n_tp
    MC = mod_shift.shape[1]
    chunk_sems = 2 * max(n_sp - 1, 1) * 3
    vm = pl.BlockSpec(memory_space=pltpu.VMEM)
    anywhere = pl.BlockSpec(memory_space=pl.ANY)
    smem = pl.BlockSpec(memory_space=pltpu.SMEM)
    dma = pltpu.SemaphoreType.DMA
    return pl.pallas_call(
        functools.partial(kernel, n_sp, n_tp, n_dp, head_width),
        out_shape=jax.ShapeDtypeStruct((R, D), latent.dtype),
        in_specs=[anywhere] * 14 + [smem, smem]
        + [anywhere] * 3,
        out_specs=vm,
        scratch_shapes=[
            pltpu.VMEM(cond.shape, BF),
            pltpu.VMEM(context_cond.shape, BF),
            pltpu.VMEM(norm_gain.shape, F32),
            pltpu.VMEM(query_gain.shape, F32),
            pltpu.VMEM(key_gain.shape, F32),
            pltpu.VMEM(value_gain.shape, F32),
            pltpu.VMEM((4, R, D), BF),
            pltpu.VMEM((C, D), BF),
            pltpu.VMEM((3,) + mod_shift.shape, BF),
            pltpu.VMEM(w_query.shape, BF),
            pltpu.VMEM(w_key.shape, BF),
            pltpu.VMEM(w_value.shape, BF),
            pltpu.VMEM((4,) + w_out.shape, BF),
            pltpu.VMEM((ROWS, 2 * head_width), F32),
            pltpu.VMEM((ROWS, 2 * head_width), F32),
            pltpu.VMEM((8, mod_shift.shape[0]), F32),
            pltpu.VMEM((8, MC), F32),
            pltpu.VMEM((max(n_sp - 1, 1), 8, MC), F32),
            pltpu.VMEM((8, MC), F32),
            pltpu.VMEM((n_tp, 8, MC), F32),
            pltpu.VMEM((8, D), F32),
            pltpu.VMEM((C + ROWS, D), BF),
            pltpu.VMEM((heads, ROWS, 2 * head_width), BF),
            pltpu.VMEM((ROWS, 2 * head_width), BF),
            pltpu.VMEM((2, 2 * ROWS, 2 * head_width), BF),
            pltpu.VMEM((heads, C + ROWS, (QW + VWALL) // heads), BF),
            pltpu.VMEM((n_sp, C + ROWS, (QW + VWALL) // heads), BF),
            pltpu.VMEM((2, 2 * ROWS, 2 * VWALL // heads), F32),
            pltpu.VMEM((2, 4, R, VWALL // heads), BF),
            pltpu.VMEM((2, 4, R, VWALL // heads), BF),
            dma((17,)),
            dma((6,)), dma((6,)),
            dma((max(n_sp - 1, 1),)), dma((max(n_sp - 1, 1),)),
            dma((3,)), dma((3,)),
            dma((chunk_sems,)), dma((chunk_sems,)),
            dma((6,)), dma((6,)),
            dma((3,)), dma((3,)),
            dma((8,)), dma((8,)),
            dma(()), dma(()),
        ],
        compiler_params=pltpu.CompilerParams(
            collective_id=0, has_side_effects=True, vmem_limit_bytes=60 * 1024 * 1024
        ),
        name="block",
    )(
        latent, context, cond, context_cond, norm_gain, mod_shift, mod_scale,
        mod_gate, w_query, w_key, w_value, query_gain, key_gain, value_gain, mix_lambda, context_lift, w_out,
        jnp.asarray(cos), jnp.asarray(sin),
    )


def solution(mesh):
    placed = (
        P(("dp", "sp", "tp"), None),
        P(("dp", "sp"), None),
        P(("dp", "sp")),
        P("sp"),
        P(),
        P("sp", "tp"),
        P("sp", "tp"),
        P("sp", "tp"),
        P(None, "tp"),
        P(None, "tp"),
        P(None, "tp"),
        P(),
        P(),
        P("tp"),
        P("tp"),
        P(),
        P("tp", None),
    )
    sizes = mesh.shape
    return jax.shard_map(
        functools.partial(on_device, sizes["sp"], sizes["tp"], sizes["dp"]),
        mesh=mesh,
        in_specs=placed,
        out_specs=P(("dp", "sp", "tp"), None),
        check_vma=False,
    )
```

```python
import functools

import jax
import jax.numpy as jnp
import numpy as np
from jax import lax
from jax.experimental import pallas as pl
from jax.experimental.pallas import tpu as pltpu
from jax.sharding import PartitionSpec as P

GRID = 64
token_eps = 0.01
head_eps = 0.001
rope_base = 10000.0
head_factor = 0.8
MESH = pl.DeviceIdType.MESH
BF = jnp.bfloat16
F32 = jnp.float32


def rope_tables(length, width):
    quarter = width // 4
    inverse = (rope_base ** (-np.arange(quarter, dtype=np.float64) / quarter)).astype(np.float32)
    pos = np.arange(length)
    row = (pos // GRID).astype(np.float32)[:, None] * inverse
    col = (pos % GRID).astype(np.float32)[:, None] * inverse
    cos = np.concatenate([np.cos(row), np.cos(row), np.cos(col), np.cos(col)], axis=1)
    sin = np.concatenate([-np.sin(row), np.sin(row), -np.sin(col), np.sin(col)], axis=1)
    return np.tile(cos, (1, 2)).astype(np.float32), np.tile(sin, (1, 2)).astype(np.float32)


def kernel(n_sp, n_tp, n_dp, head_width, *refs):
    (
        lat_h, ctx_h, cond_h, cctx_h, gain_h, ms_h, msc_h, mg_h, wq_h, wk_h, wv_h,
        qg_h, kg_h, vg_h, lam_r, lift_r, wo_h, cos_h, sin_h,
        out_r,
        cond_r, cctx_r, gain_r, qg_r, kg_r, vg_r,
        lat, ctx, mw, wq, wk, wv, wo, cosv, sinv,
        act, part, mod_in, summed, mod_full, vecs, invs, normed, qown, qin, qm, kvl, kvr, acc, mine, ho,
        loc, bs_lat, br_lat, bs_mod, br_mod, bs_mt, br_mt, bs_kv, br_kv, bs_wo, br_wo,
        bs_dd, br_dd, bs_ho, br_ho, bs_q, br_q,
    ) = refs
    s = lax.axis_index("sp")
    t = lax.axis_index("tp")
    d_ix = lax.axis_index("dp")
    core = lax.rem(d_ix, 2)
    partner = d_ix + 1 - 2 * core
    t_odd = lax.rem(t, 2)
    nbr1 = t + 1 - 2 * t_odd
    nbr2 = lax.rem(t + 2, 4)
    nbr3 = lax.rem(nbr1 + 2, 4)
    peers = (t, nbr1, nbr2, nbr3)
    e = lax.rem(s, 2)
    pair = s + 1 - 2 * e
    R = lat.shape[1]
    HR = R // 2
    C = ctx.shape[0]
    D = lat.shape[2]
    QW = wq.shape[1]
    n_head = QW // (2 * head_width)
    HW = 2 * head_width
    VW = wv.shape[1] // n_head
    ROWS = 4 * R

    def local(i, src, dst):
        c = pltpu.make_async_copy(src, dst, loc.at[i])
        c.start()
        return c

    l_one = [
        local(11 + j, src, dst)
        for j, (src, dst) in enumerate(
            ((cond_h, cond_r), (cctx_h, cctx_r), (gain_h, gain_r), (qg_h, qg_r), (kg_h, kg_r),
             (vg_h, vg_r))
        )
    ]
    l_lat = local(0, lat_h, lat.at[0])
    l_mod = [local(1 + j, h, mw.at[j]) for j, h in enumerate((ms_h, msc_h, mg_h))]
    l_ctx = local(4, ctx_h, ctx)
    l_wk = local(5, wk_h, wk)
    l_wv = local(6, wv_h, wv)
    l_wq = local(7, wq_h, wq)
    l_wo = local(8, wo_h, wo.at[0])
    l_cos = local(9, cos_h.at[pl.ds(s * ROWS, ROWS)], cosv)
    l_sin = local(10, sin_h.at[pl.ds(s * ROWS, ROWS)], sinv)

    bar = pltpu.get_barrier_semaphore()
    for k in range(1, n_sp):
        pl.semaphore_signal(bar, inc=1, device_id={"sp": lax.rem(s + k, n_sp)}, device_id_type=MESH)
    for k in range(1, 4):
        pl.semaphore_signal(bar, inc=1, device_id={"tp": peers[k]}, device_id_type=MESH)
        pl.semaphore_signal(
            bar, inc=1, device_id={"sp": pair, "tp": peers[k]}, device_id_type=MESH
        )
    pl.semaphore_signal(bar, inc=1, device_id={"dp": partner}, device_id_type=MESH)

    act[...] = jnp.zeros_like(act)
    for row, ref in ((0, cond_r), (1, cctx_r)):
        l_one[row].wait()
        v = ref[...].astype(F32).reshape(1, -1)
        act[row : row + 1, :] = v / (1.0 + jnp.exp(-v))
    acts = act[...].astype(BF)
    part[...] = jnp.zeros_like(part)
    for j in range(3):
        l_mod[j].wait()
        res = jnp.dot(acts, mw[j], preferred_element_type=F32)
        part[2 * j : 2 * j + 2, :] = res[0:2]

    pl.semaphore_wait(bar, n_sp + 6)

    def remote(src, dst, ss, rs, where):
        return pltpu.make_async_remote_copy(
            src_ref=src, dst_ref=dst, send_sem=ss, recv_sem=rs, device_id=where, device_id_type=MESH
        )

    mod_copies = []
    for k in range(1, n_sp):
        c = remote(part, mod_in.at[k - 1], bs_mod.at[k - 1], br_mod.at[k - 1],
                   {"sp": lax.rem(s + k, n_sp)})
        c.start()
        mod_copies.append(c)

    l_lat.wait()

    def lat_copy(i, src_slot, dst_slot, half, where):
        rows = pl.ds(half * HR, HR)
        return remote(lat.at[src_slot, rows], lat.at[dst_slot, rows], bs_lat.at[i], br_lat.at[i],
                      {"tp": where})

    x0 = lat_copy(0, 0, 1, 0, nbr1)
    y1 = lat_copy(1, 0, 2, 1, nbr2)
    x1 = lat_copy(2, 0, 1, 1, nbr1)
    y0 = lat_copy(3, 0, 2, 0, nbr2)
    f0 = lat_copy(4, 1, 3, 0, nbr2)
    f1 = lat_copy(5, 2, 3, 1, nbr1)
    for c in (x0, y1):
        c.start()

    l_ctx.wait()

    def inverse_rows(src, count, dst_at):
        for i in range(count // 16):
            v = src[i * 16 : (i + 1) * 16, :].astype(F32)
            inv = lax.rsqrt(jnp.mean(v * v, axis=-1, keepdims=True) + token_eps)
            invs[dst_at + i * 16 : dst_at + (i + 1) * 16, :] = jnp.broadcast_to(inv, (16, 128))

    inverse_rows(ctx, C, 0)
    inverse_rows(lat.at[0], R, C)

    total = part[...]
    for k in range(n_sp - 1):
        mod_copies[k].wait_recv()
        total = total + mod_in[k]
    summed[...] = total
    mod_full[t] = total
    tp_copies = []
    for k in range(1, 4):
        c = remote(summed, mod_full.at[t], bs_mt.at[k - 1], br_mt.at[k - 1], {"tp": peers[k]})
        c.start()
        tp_copies.append(c)
    x1.start()
    y0.start()
    x0.wait_recv()
    f0.start()
    y1.wait_recv()
    f1.start()

    for k in range(1, 4):
        remote(summed, mod_full.at[peers[k]], bs_mt.at[k - 1], br_mt.at[k - 1],
               {"tp": peers[k]}).wait_recv()

    def full_row(j):
        return jnp.concatenate([mod_full[q, j : j + 1, :] for q in range(n_tp)], axis=1)

    for c in l_one[2:]:
        c.wait()
    gain = gain_r[...].reshape(1, -1)
    q_gain = qg_r[...].reshape(1, -1)
    q_gain = jnp.concatenate([q_gain, q_gain], axis=1)
    k_gain = kg_r[...].reshape(1, -1)
    k_gain = jnp.concatenate([k_gain, k_gain], axis=1)
    v_gain = vg_r[...].reshape(1, -1)
    vecs[0:1, :] = full_row(0)
    vecs[1:2, :] = full_row(1)
    vecs[2:3, :] = gain * (1.0 + full_row(2))
    vecs[3:4, :] = gain * (1.0 + full_row(3))
    vecs[4:5, :] = full_row(4)

    HALF = wo.shape[1] // 2
    QUART = HALF // 2

    def wo_rows(q):
        return pl.ds(pl.multiple_of(core * HALF + q * QUART, QUART), QUART)

    def wo_copy(i, src_slot, dst_slot, q, where):
        return remote(wo.at[src_slot, wo_rows(q)], wo.at[dst_slot, wo_rows(q)], bs_wo.at[i],
                      br_wo.at[i], {"tp": where})

    def dd_copy(k):
        rows = pl.ds(pl.multiple_of(core * HALF, HALF), HALF)
        return remote(wo.at[k, rows], wo.at[k, rows], bs_dd.at[k - 1], br_dd.at[k - 1],
                      {"dp": partner})

    def dd_recv(k):
        rows = pl.ds(pl.multiple_of((1 - core) * HALF, HALF), HALF)
        return remote(wo.at[k, rows], wo.at[k, rows], bs_dd.at[k - 1], br_dd.at[k - 1],
                      {"dp": partner})

    wx0 = wo_copy(0, 0, 1, 0, nbr1)
    wy1 = wo_copy(1, 0, 2, 1, nbr2)
    wx1 = wo_copy(2, 0, 1, 1, nbr1)
    wy0 = wo_copy(3, 0, 2, 0, nbr2)
    wf0 = wo_copy(4, 1, 3, 0, nbr2)
    wf1 = wo_copy(5, 2, 3, 1, nbr1)

    def norm_rows(src, row, count, dst_at):
        step = 16

        @pl.loop(0, count // step, unroll=True)
        def _(i):
            at = pl.multiple_of(i * step, step)
            v = src[pl.ds(at, step), :].astype(F32)
            inv = lax.rsqrt(jnp.mean(v * v, axis=-1, keepdims=True) + token_eps)
            normed[pl.ds(dst_at + at, step), :] = (
                v * inv * vecs[2 + row : 3 + row, :] + vecs[row : row + 1, :]
            ).astype(BF)

    def apply_rows(src, row, count, dst_at):
        for i in range(count // 16):
            v = src[i * 16 : (i + 1) * 16, :].astype(F32)
            at = slice(dst_at + i * 16, dst_at + (i + 1) * 16)
            normed[at, :] = (
                v * invs[at, 0:1] * vecs[2 + row : 3 + row, :] + vecs[row : row + 1, :]
            ).astype(BF)

    group = (
        lax.broadcasted_iota(jnp.int32, (QW, QW), 0) // head_width
        == lax.broadcasted_iota(jnp.int32, (QW, QW), 1) // head_width
    )
    group = jnp.where(group, 1.0 / head_width, 0.0).astype(F32)

    def head_norm(x):
        mean = jnp.dot(x * x, group, precision=lax.Precision.HIGHEST, preferred_element_type=F32)
        return x * lax.rsqrt(mean + token_eps)

    def turn(y, cos, sin):
        lane = lax.broadcasted_iota(jnp.int32, y.shape, 1)
        front = lax.rem(lane, head_width // 2) < head_width // 4
        other = jnp.where(
            front,
            pltpu.roll(y, HW - head_width // 4, axis=1),
            pltpu.roll(y, head_width // 4, axis=1),
        )
        return y * cos + other * sin

    def project_block(k, first):
        rows = pl.ds(first + C, R)
        x = normed[C + k * R : C + (k + 1) * R, :]
        at = pl.ds(pl.multiple_of(peers[k] * R, R), R)
        cos, sin = cosv[at, :], sinv[at, :]
        kk = head_norm(jnp.dot(x, wk[...], preferred_element_type=F32))
        for h in range(n_head):
            y = kk[:, h * HW : (h + 1) * HW] * k_gain
            kvl[h, rows, 0:HW] = turn(y, cos, sin).astype(BF)
        vv = jnp.dot(x, wv[...], preferred_element_type=F32).astype(BF)
        for h in range(n_head):
            kvl[h, rows, HW:] = vv[:, h * VW : (h + 1) * VW]

    def project_queries():
        x = normed[C:, :]
        qq = head_norm(jnp.dot(x, wq[...], preferred_element_type=F32))
        for k in range(4):
            at = pl.ds(pl.multiple_of(peers[k] * R, R), R)
            cos, sin = cosv[at, :], sinv[at, :]
            for h in range(n_head):
                y = qq[k * R : (k + 1) * R, h * HW : (h + 1) * HW] * q_gain
                qown[h, k * R : (k + 1) * R, :] = (
                    turn(y, cos, sin) * (head_width ** -0.5)
                ).astype(BF)

    def split_maps(q, at):
        lane = lax.broadcasted_iota(jnp.int32, q.shape, 1)
        for m in range(2):
            qm[m, at : at + ROWS, :] = jnp.where(lane // head_width == m, q, jnp.zeros_like(q))

    chunks = ((0, C + R), (C + R, 2 * R), (C + 3 * R, R))

    def kv_copy(direction, dist, c, src, origin, where):
        at, count = chunks[c]
        i = (direction * (n_sp - 1) + dist - 1) * len(chunks) + c
        return remote(src.at[pl.ds(at, count)], kvr.at[origin, pl.ds(at, count)], bs_kv.at[i],
                      br_kv.at[i], {"sp": where})

    def side(direction, dist, c, act_on):
        sign = 1 - 2 * direction
        hop = 1 if dist == 1 else 2
        origin = s - sign * (dist - hop)
        where = s + sign * hop
        ok = jnp.logical_and(
            jnp.logical_and(origin >= 0, origin < n_sp),
            jnp.logical_and(where >= 0, where < n_sp),
        )

        @pl.when(ok)
        def _():
            if dist == 1:
                src = kvl.at[1 - e]
            elif dist == 2:
                src = kvl.at[e]
            else:
                src = kvr.at[origin]
            act_on(kv_copy(direction, dist, c, src, origin, where))

    def start(copy):
        copy.start()

    def drain(copy):
        copy.wait_send()

    def send_own(c):
        for dist in (1, 2):
            if dist < n_sp:
                for direction in (0, 1):
                    side(direction, dist, c, start)

    apply_rows(ctx, 1, C, 0)
    apply_rows(lat.at[0], 0, R, C)
    l_wk.wait()
    l_wv.wait()
    l_cos.wait()
    l_sin.wait()
    x = normed[0:C, :]
    kk = head_norm(jnp.dot(x, wk[...], preferred_element_type=F32))
    vv = jnp.dot(x, wv[...], preferred_element_type=F32).astype(BF)
    for h in range(n_head):
        kvl[h, 0:C, 0:HW] = (kk[:, h * HW : (h + 1) * HW] * k_gain).astype(BF)
        kvl[h, 0:C, HW:] = vv[:, h * VW : (h + 1) * VW]
    project_block(0, 0)
    send_own(0)

    x1.wait_recv()
    y0.wait_recv()
    l_wo.wait()
    for c in (wx0, wy1, wx1, wy0):
        c.start()
    norm_rows(lat.at[1], 0, R, C + R)
    norm_rows(lat.at[2], 0, R, C + 2 * R)
    project_block(1, R)
    project_block(2, 2 * R)
    send_own(1)
    f0.wait_recv()
    f1.wait_recv()
    norm_rows(lat.at[3], 0, R, C + 3 * R)
    project_block(3, 3 * R)
    send_own(2)

    def arrive(dist, c):
        for direction in (0, 1):
            origin = s - dist if direction == 0 else s + dist
            here = origin >= 0 if direction == 0 else origin < n_sp

            @pl.when(here)
            def _():
                kv_copy(direction, dist, c, kvr.at[origin], origin, s).wait_recv()

            if dist + 2 < n_sp:
                side(direction, dist + 2, c, start)

    l_wq.wait()
    project_queries()
    q_copy = remote(qown.at[1 - e], qin, bs_q, br_q, {"sp": pair})
    q_copy.start()
    split_maps(qown[e], 0)
    arrive(1, 0)

    QB = 2 * R
    lift = lift_r[e]

    def attend(block, at, keys, start_row, count, first):
        k = block[at : at + keys, 0:HW]
        v = block[at : at + keys, HW:]
        vx = jnp.concatenate([v, jnp.ones_like(v)], axis=1)
        key = lax.broadcasted_iota(jnp.int32, (1, keys), 1)
        for m in range(2):
            for b in range(count // QB):
                rows = slice(start_row + b * QB, start_row + (b + 1) * QB)
                sc = lax.dot_general(
                    qm[m, rows, :], k, (((1,), (1,)), ((), ())), preferred_element_type=F32
                )
                if at < C:
                    sc = sc + jnp.where(key < C - at, lift, 0.0)
                p = jnp.exp(sc).astype(BF)
                add = jnp.dot(p, vx, preferred_element_type=F32)
                if first:
                    acc[m, rows, :] = add
                else:
                    acc[m, rows, :] += add

    def attend_arrived(dist, at, keys):
        @pl.when(s - dist >= 0)
        def _():
            attend(kvr.at[s - dist], at, keys, 0, 2 * ROWS, False)

        @pl.when(s + dist < n_sp)
        def _():
            attend(kvr.at[s + dist], at, keys, 0, 2 * ROWS, False)

    attend(kvl.at[e], 0, C + ROWS, 0, ROWS, True)
    for c in range(1, len(chunks)):
        arrive(1, c)
    wx0.wait_recv()
    wf0.start()
    wy1.wait_recv()
    wf1.start()
    q_copy.wait_recv()
    split_maps(qin[...], ROWS)
    attend(kvl.at[e], 0, C + ROWS, ROWS, ROWS, True)

    for dist in range(1, n_sp):
        last = dist == n_sp - 1
        if dist > 1:
            for c in range(len(chunks)):
                arrive(dist, c)
                if last:
                    attend_arrived(dist, *chunks[c])
        if not last:
            attend_arrived(dist, 0, C + ROWS)
        if dist == 2 or (last and n_sp == 2):
            wx1.wait_recv()
            dd_copy(1).start()
            wy0.wait_recv()
            dd_copy(2).start()

    def ho_copy(q, k):
        i = q * 4 + k
        where = {"tp": peers[k]} if q == 0 else {"sp": pair, "tp": peers[k]}
        if q == 1 and k == 0:
            where = {"sp": pair}
        return remote(mine.at[q, k], ho.at[q, k], bs_ho.at[i], br_ho.at[i], where)

    for q, k in ((1, 3), (1, 1), (1, 2), (0, 3), (1, 0), (0, 1), (0, 2), (0, 0)):
        rows = slice((4 * q + k) * R, (4 * q + k + 1) * R)
        a0 = acc[0, rows, :]
        a1 = acc[1, rows, :]
        mixed = a0[:, :VW] / a0[:, VW:] - lam_r[e] * (a1[:, :VW] / a1[:, VW:])
        inv = lax.rsqrt(jnp.mean(mixed * mixed, axis=-1, keepdims=True) + head_eps)
        mine[q, k, :, :] = (mixed * inv * v_gain * head_factor).astype(BF)
        if q or k:
            ho_copy(q, k).start()

    wf0.wait_recv()
    wf1.wait_recv()
    dd_copy(3).start()

    def head_rows(q):
        return pl.ds(pl.multiple_of((e if q == 0 else 1 - e) * VW, VW), VW)

    out = jnp.dot(mine[0, 0], wo[0, head_rows(0), :], preferred_element_type=F32)
    for q, k in ((0, 1), (0, 2), (1, 0), (0, 3), (1, 1), (1, 2), (1, 3)):
        if q == 0:
            dd_recv(k).wait_recv()
        ho_copy(q, k).wait_recv()
        out += jnp.dot(ho[q, k], wo[k, head_rows(q), :], preferred_element_type=F32)
    out_r[...] = vecs[4:5, :] * out

    for c in mod_copies + tp_copies + [x0, y1, x1, y0, f0, f1, wx0, wy1, wx1, wy0, wf0, wf1]:
        c.wait_send()
    for k in range(1, 4):
        dd_copy(k).wait_send()
    q_copy.wait_send()
    for q in range(2):
        for k in range(4):
            if q or k:
                ho_copy(q, k).wait_send()
    for dist in range(1, n_sp):
        for c in range(len(chunks)):
            for direction in (0, 1):
                side(direction, dist, c, drain)


def on_device(n_sp, n_tp, n_dp, *args):
    (
        latent, context, cond, context_cond, norm_gain, mod_shift, mod_scale, mod_gate,
        w_query, w_key, w_value, query_gain, key_gain, mix_lambda, context_lift, value_gain, w_out,
    ) = args
    R, D = latent.shape
    C = context.shape[0]
    head_width = query_gain.shape[0]
    cos, sin = rope_tables(R * n_sp * n_tp, head_width)
    QW, VWALL = w_query.shape[1], w_value.shape[1]
    heads = mix_lambda.shape[0]
    ROWS = R * n_tp
    MC = mod_shift.shape[1]
    chunk_sems = 2 * max(n_sp - 1, 1) * 3
    vm = pl.BlockSpec(memory_space=pltpu.VMEM)
    anywhere = pl.BlockSpec(memory_space=pl.ANY)
    smem = pl.BlockSpec(memory_space=pltpu.SMEM)
    dma = pltpu.SemaphoreType.DMA
    update = pl.pallas_call(
        functools.partial(kernel, n_sp, n_tp, n_dp, head_width),
        out_shape=jax.ShapeDtypeStruct((R, D), F32),
        in_specs=[anywhere] * 14 + [smem, smem]
        + [anywhere] * 3,
        out_specs=vm,
        scratch_shapes=[
            pltpu.VMEM(cond.shape, BF),
            pltpu.VMEM(context_cond.shape, BF),
            pltpu.VMEM(norm_gain.shape, F32),
            pltpu.VMEM(query_gain.shape, F32),
            pltpu.VMEM(key_gain.shape, F32),
            pltpu.VMEM(value_gain.shape, F32),
            pltpu.VMEM((4, R, D), BF),
            pltpu.VMEM((C, D), BF),
            pltpu.VMEM((3,) + mod_shift.shape, BF),
            pltpu.VMEM(w_query.shape, BF),
            pltpu.VMEM(w_key.shape, BF),
            pltpu.VMEM(w_value.shape, BF),
            pltpu.VMEM((4,) + w_out.shape, BF),
            pltpu.VMEM((ROWS, 2 * head_width), F32),
            pltpu.VMEM((ROWS, 2 * head_width), F32),
            pltpu.VMEM((8, mod_shift.shape[0]), F32),
            pltpu.VMEM((8, MC), F32),
            pltpu.VMEM((max(n_sp - 1, 1), 8, MC), F32),
            pltpu.VMEM((8, MC), F32),
            pltpu.VMEM((n_tp, 8, MC), F32),
            pltpu.VMEM((8, D), F32),
            pltpu.VMEM((C + R, 128), F32),
            pltpu.VMEM((C + ROWS, D), BF),
            pltpu.VMEM((heads, ROWS, 2 * head_width), BF),
            pltpu.VMEM((ROWS, 2 * head_width), BF),
            pltpu.VMEM((2, 2 * ROWS, 2 * head_width), BF),
            pltpu.VMEM((heads, C + ROWS, (QW + VWALL) // heads), BF),
            pltpu.VMEM((n_sp, C + ROWS, (QW + VWALL) // heads), BF),
            pltpu.VMEM((2, 2 * ROWS, 2 * VWALL // heads), F32),
            pltpu.VMEM((2, 4, R, VWALL // heads), BF),
            pltpu.VMEM((2, 4, R, VWALL // heads), BF),
            dma((17,)),
            dma((6,)), dma((6,)),
            dma((max(n_sp - 1, 1),)), dma((max(n_sp - 1, 1),)),
            dma((3,)), dma((3,)),
            dma((chunk_sems,)), dma((chunk_sems,)),
            dma((6,)), dma((6,)),
            dma((3,)), dma((3,)),
            dma((8,)), dma((8,)),
            dma(()), dma(()),
        ],
        compiler_params=pltpu.CompilerParams(
            collective_id=0, has_side_effects=True, vmem_limit_bytes=60 * 1024 * 1024
        ),
        name="block",
    )(
        latent, context, cond, context_cond, norm_gain, mod_shift, mod_scale,
        mod_gate, w_query, w_key, w_value, query_gain, key_gain, value_gain, mix_lambda, context_lift, w_out,
        jnp.asarray(cos), jnp.asarray(sin),
    )
    return (latent.astype(F32) + update).astype(latent.dtype)


def solution(mesh):
    placed = (
        P(("dp", "sp", "tp"), None),
        P(("dp", "sp"), None),
        P(("dp", "sp")),
        P("sp"),
        P(),
        P("sp", "tp"),
        P("sp", "tp"),
        P("sp", "tp"),
        P(None, "tp"),
        P(None, "tp"),
        P(None, "tp"),
        P(),
        P(),
        P("tp"),
        P("tp"),
        P(),
        P("tp", None),
    )
    sizes = mesh.shape
    return jax.shard_map(
        functools.partial(on_device, sizes["sp"], sizes["tp"], sizes["dp"]),
        mesh=mesh,
        in_specs=placed,
        out_specs=P(("dp", "sp", "tp"), None),
        check_vma=False,
    )
```

```python
import functools

import jax
import jax.numpy as jnp
import numpy as np
from jax import lax
from jax.experimental import pallas as pl
from jax.experimental.pallas import tpu as pltpu
from jax.sharding import PartitionSpec as P

GRID = 64
token_eps = 0.01
head_eps = 0.001
rope_base = 10000.0
head_factor = 0.8
MESH = pl.DeviceIdType.MESH
BF = jnp.bfloat16
F32 = jnp.float32


def rope_tables(length, width):
    quarter = width // 4
    inverse = (rope_base ** (-np.arange(quarter, dtype=np.float64) / quarter)).astype(np.float32)
    pos = np.arange(length)
    row = (pos // GRID).astype(np.float32)[:, None] * inverse
    col = (pos % GRID).astype(np.float32)[:, None] * inverse
    cos = np.concatenate([np.cos(row), np.cos(row), np.cos(col), np.cos(col)], axis=1)
    sin = np.concatenate([-np.sin(row), np.sin(row), -np.sin(col), np.sin(col)], axis=1)
    return np.tile(cos, (1, 2)).astype(np.float32), np.tile(sin, (1, 2)).astype(np.float32)


def kernel(n_sp, n_tp, n_dp, head_width, *refs):
    (
        lat_h, ctx_h, cond_h, cctx_h, gain_h, ms_h, msc_h, mg_h, wq_h, wk_h, wv_h,
        qg_h, kg_h, vg_h, lam_r, lift_r, wo_h, cos_h, sin_h,
        out_r,
        cond_r, cctx_r, gain_r, qg_r, kg_r, vg_r,
        lat, ctx, mw, wq, wk, wv, wo, cosv, sinv,
        act, part, mod_in, summed, mod_full, vecs, invs, normed, qown, qin, qm, kvl, kvr, acc, mine, ho,
        loc, bs_lat, br_lat, bs_mod, br_mod, bs_mt, br_mt, bs_kv, br_kv, bs_wo, br_wo,
        bs_dd, br_dd, bs_ho, br_ho, bs_q, br_q,
    ) = refs
    s = lax.axis_index("sp")
    t = lax.axis_index("tp")
    d_ix = lax.axis_index("dp")
    core = lax.rem(d_ix, 2)
    partner = d_ix + 1 - 2 * core
    t_odd = lax.rem(t, 2)
    nbr1 = t + 1 - 2 * t_odd
    nbr2 = lax.rem(t + 2, 4)
    nbr3 = lax.rem(nbr1 + 2, 4)
    peers = (t, nbr1, nbr2, nbr3)
    e = lax.rem(s, 2)
    pair = s + 1 - 2 * e
    R = lat.shape[1]
    HR = R // 2
    C = ctx.shape[0]
    D = lat.shape[2]
    QW = wq.shape[1]
    n_head = QW // (2 * head_width)
    HW = 2 * head_width
    VW = wv.shape[1] // n_head
    ROWS = 4 * R

    def local(i, src, dst):
        c = pltpu.make_async_copy(src, dst, loc.at[i])
        c.start()
        return c

    l_one = [
        local(11 + j, src, dst)
        for j, (src, dst) in enumerate(
            ((cond_h, cond_r), (cctx_h, cctx_r), (gain_h, gain_r), (qg_h, qg_r), (kg_h, kg_r),
             (vg_h, vg_r))
        )
    ]
    l_lat = local(0, lat_h, lat.at[0])
    l_mod = [local(1 + j, h, mw.at[j]) for j, h in enumerate((ms_h, msc_h, mg_h))]
    l_ctx = local(4, ctx_h, ctx)
    l_wk = local(5, wk_h, wk)
    l_wv = local(6, wv_h, wv)
    l_wq = local(7, wq_h, wq)
    l_wo = local(8, wo_h, wo.at[0])
    l_cos = local(9, cos_h.at[pl.ds(s * ROWS, ROWS)], cosv)
    l_sin = local(10, sin_h.at[pl.ds(s * ROWS, ROWS)], sinv)

    bar = pltpu.get_barrier_semaphore()
    for k in range(1, n_sp):
        pl.semaphore_signal(bar, inc=1, device_id={"sp": lax.rem(s + k, n_sp)}, device_id_type=MESH)
    for k in range(1, 4):
        pl.semaphore_signal(bar, inc=1, device_id={"tp": peers[k]}, device_id_type=MESH)
        pl.semaphore_signal(
            bar, inc=1, device_id={"sp": pair, "tp": peers[k]}, device_id_type=MESH
        )
    pl.semaphore_signal(bar, inc=1, device_id={"dp": partner}, device_id_type=MESH)

    act[...] = jnp.zeros_like(act)
    for row, ref in ((0, cond_r), (1, cctx_r)):
        l_one[row].wait()
        v = ref[...].astype(F32).reshape(1, -1)
        act[row : row + 1, :] = v / (1.0 + jnp.exp(-v))
    acts = act[...].astype(BF)
    part[...] = jnp.zeros_like(part)
    for j in range(3):
        l_mod[j].wait()
        res = jnp.dot(acts, mw[j], preferred_element_type=F32)
        part[2 * j : 2 * j + 2, :] = res[0:2]

    pl.semaphore_wait(bar, n_sp + 6)

    def remote(src, dst, ss, rs, where):
        return pltpu.make_async_remote_copy(
            src_ref=src, dst_ref=dst, send_sem=ss, recv_sem=rs, device_id=where, device_id_type=MESH
        )

    mod_copies = []
    for k in range(1, n_sp):
        c = remote(part, mod_in.at[k - 1], bs_mod.at[k - 1], br_mod.at[k - 1],
                   {"sp": lax.rem(s + k, n_sp)})
        c.start()
        mod_copies.append(c)

    l_lat.wait()

    def lat_copy(i, src_slot, dst_slot, half, where):
        rows = pl.ds(half * HR, HR)
        return remote(lat.at[src_slot, rows], lat.at[dst_slot, rows], bs_lat.at[i], br_lat.at[i],
                      {"tp": where})

    x0 = lat_copy(0, 0, 1, 0, nbr1)
    y1 = lat_copy(1, 0, 2, 1, nbr2)
    x1 = lat_copy(2, 0, 1, 1, nbr1)
    y0 = lat_copy(3, 0, 2, 0, nbr2)
    f0 = lat_copy(4, 1, 3, 0, nbr2)
    f1 = lat_copy(5, 2, 3, 1, nbr1)
    for c in (x0, y1):
        c.start()

    l_ctx.wait()

    def inverse_rows(src, count, dst_at):
        for i in range(count // 16):
            v = src[i * 16 : (i + 1) * 16, :].astype(F32)
            inv = lax.rsqrt(jnp.mean(v * v, axis=-1, keepdims=True) + token_eps)
            invs[dst_at + i * 16 : dst_at + (i + 1) * 16, :] = jnp.broadcast_to(inv, (16, 128))

    inverse_rows(ctx, C, 0)
    inverse_rows(lat.at[0], R, C)

    total = part[...]
    for k in range(n_sp - 1):
        mod_copies[k].wait_recv()
        total = total + mod_in[k]
    summed[...] = total
    mod_full[t] = total
    tp_copies = []
    for k in range(1, 4):
        c = remote(summed, mod_full.at[t], bs_mt.at[k - 1], br_mt.at[k - 1], {"tp": peers[k]})
        c.start()
        tp_copies.append(c)
    x1.start()
    y0.start()
    x0.wait_recv()
    f0.start()
    y1.wait_recv()
    f1.start()

    for k in range(1, 4):
        remote(summed, mod_full.at[peers[k]], bs_mt.at[k - 1], br_mt.at[k - 1],
               {"tp": peers[k]}).wait_recv()

    def full_row(j):
        return jnp.concatenate([mod_full[q, j : j + 1, :] for q in range(n_tp)], axis=1)

    for c in l_one[2:]:
        c.wait()
    gain = gain_r[...].reshape(1, -1)
    q_gain = qg_r[...].reshape(1, -1)
    q_gain = jnp.concatenate([q_gain, q_gain], axis=1)
    k_gain = kg_r[...].reshape(1, -1)
    k_gain = jnp.concatenate([k_gain, k_gain], axis=1)
    v_gain = vg_r[...].reshape(1, -1)
    vecs[0:1, :] = full_row(0)
    vecs[1:2, :] = full_row(1)
    vecs[2:3, :] = gain * (1.0 + full_row(2))
    vecs[3:4, :] = gain * (1.0 + full_row(3))
    vecs[4:5, :] = full_row(4)

    HALF = wo.shape[1] // 2
    QUART = HALF // 2

    def wo_rows(q):
        return pl.ds(pl.multiple_of(core * HALF + q * QUART, QUART), QUART)

    def wo_copy(i, src_slot, dst_slot, q, where):
        return remote(wo.at[src_slot, wo_rows(q)], wo.at[dst_slot, wo_rows(q)], bs_wo.at[i],
                      br_wo.at[i], {"tp": where})

    def dd_copy(k):
        rows = pl.ds(pl.multiple_of(core * HALF, HALF), HALF)
        return remote(wo.at[k, rows], wo.at[k, rows], bs_dd.at[k - 1], br_dd.at[k - 1],
                      {"dp": partner})

    def dd_recv(k):
        rows = pl.ds(pl.multiple_of((1 - core) * HALF, HALF), HALF)
        return remote(wo.at[k, rows], wo.at[k, rows], bs_dd.at[k - 1], br_dd.at[k - 1],
                      {"dp": partner})

    wx0 = wo_copy(0, 0, 1, 0, nbr1)
    wy1 = wo_copy(1, 0, 2, 1, nbr2)
    wx1 = wo_copy(2, 0, 1, 1, nbr1)
    wy0 = wo_copy(3, 0, 2, 0, nbr2)
    wf0 = wo_copy(4, 1, 3, 0, nbr2)
    wf1 = wo_copy(5, 2, 3, 1, nbr1)

    def norm_rows(src, row, count, dst_at):
        step = 16

        @pl.loop(0, count // step, unroll=True)
        def _(i):
            at = pl.multiple_of(i * step, step)
            v = src[pl.ds(at, step), :].astype(F32)
            inv = lax.rsqrt(jnp.mean(v * v, axis=-1, keepdims=True) + token_eps)
            normed[pl.ds(dst_at + at, step), :] = (
                v * inv * vecs[2 + row : 3 + row, :] + vecs[row : row + 1, :]
            ).astype(BF)

    def apply_rows(src, row, count, dst_at):
        for i in range(count // 16):
            v = src[i * 16 : (i + 1) * 16, :].astype(F32)
            at = slice(dst_at + i * 16, dst_at + (i + 1) * 16)
            normed[at, :] = (
                v * invs[at, 0:1] * vecs[2 + row : 3 + row, :] + vecs[row : row + 1, :]
            ).astype(BF)

    group = (
        lax.broadcasted_iota(jnp.int32, (QW, QW), 0) // head_width
        == lax.broadcasted_iota(jnp.int32, (QW, QW), 1) // head_width
    )
    group = jnp.where(group, 1.0 / head_width, 0.0).astype(F32)

    def head_norm(x):
        mean = jnp.dot(x * x, group, precision=lax.Precision.HIGHEST, preferred_element_type=F32)
        return x * lax.rsqrt(mean + token_eps)

    def turn(y, cos, sin):
        lane = lax.broadcasted_iota(jnp.int32, y.shape, 1)
        front = lax.rem(lane, head_width // 2) < head_width // 4
        other = jnp.where(
            front,
            pltpu.roll(y, HW - head_width // 4, axis=1),
            pltpu.roll(y, head_width // 4, axis=1),
        )
        return y * cos + other * sin

    def project_block(k, first):
        rows = pl.ds(first + C, R)
        x = normed[C + k * R : C + (k + 1) * R, :]
        at = pl.ds(pl.multiple_of(peers[k] * R, R), R)
        cos, sin = cosv[at, :], sinv[at, :]
        kk = head_norm(jnp.dot(x, wk[...], preferred_element_type=F32))
        for h in range(n_head):
            y = kk[:, h * HW : (h + 1) * HW] * k_gain
            kvl[h, rows, 0:HW] = turn(y, cos, sin).astype(BF)
        vv = jnp.dot(x, wv[...], preferred_element_type=F32).astype(BF)
        for h in range(n_head):
            kvl[h, rows, HW:] = vv[:, h * VW : (h + 1) * VW]

    def project_queries():
        x = normed[C:, :]
        qq = head_norm(jnp.dot(x, wq[...], preferred_element_type=F32))
        for k in range(4):
            at = pl.ds(pl.multiple_of(peers[k] * R, R), R)
            cos, sin = cosv[at, :], sinv[at, :]
            for h in range(n_head):
                y = qq[k * R : (k + 1) * R, h * HW : (h + 1) * HW] * q_gain
                qown[h, k * R : (k + 1) * R, :] = (
                    turn(y, cos, sin) * (head_width ** -0.5)
                ).astype(BF)

    def split_maps(q, at):
        lane = lax.broadcasted_iota(jnp.int32, q.shape, 1)
        for m in range(2):
            qm[m, at : at + ROWS, :] = jnp.where(lane // head_width == m, q, jnp.zeros_like(q))

    chunks = ((0, C + R), (C + R, 2 * R), (C + 3 * R, R))

    def kv_copy(direction, dist, c, src, origin, where):
        at, count = chunks[c]
        i = (direction * (n_sp - 1) + dist - 1) * len(chunks) + c
        return remote(src.at[pl.ds(at, count)], kvr.at[origin, pl.ds(at, count)], bs_kv.at[i],
                      br_kv.at[i], {"sp": where})

    def side(direction, dist, c, act_on):
        sign = 1 - 2 * direction
        hop = 1 if dist == 1 else 2
        origin = s - sign * (dist - hop)
        where = s + sign * hop
        ok = jnp.logical_and(
            jnp.logical_and(origin >= 0, origin < n_sp),
            jnp.logical_and(where >= 0, where < n_sp),
        )

        @pl.when(ok)
        def _():
            if dist == 1:
                src = kvl.at[1 - e]
            elif dist == 2:
                src = kvl.at[e]
            else:
                src = kvr.at[origin]
            act_on(kv_copy(direction, dist, c, src, origin, where))

    def start(copy):
        copy.start()

    def drain(copy):
        copy.wait_send()

    def send_own(c):
        for dist in (1, 2):
            if dist < n_sp:
                for direction in (0, 1):
                    side(direction, dist, c, start)

    apply_rows(ctx, 1, C, 0)
    apply_rows(lat.at[0], 0, R, C)
    l_wk.wait()
    l_wv.wait()
    l_cos.wait()
    l_sin.wait()
    x = normed[0:C, :]
    kk = head_norm(jnp.dot(x, wk[...], preferred_element_type=F32))
    vv = jnp.dot(x, wv[...], preferred_element_type=F32).astype(BF)
    for h in range(n_head):
        kvl[h, 0:C, 0:HW] = (kk[:, h * HW : (h + 1) * HW] * k_gain).astype(BF)
        kvl[h, 0:C, HW:] = vv[:, h * VW : (h + 1) * VW]
    project_block(0, 0)
    send_own(0)

    x1.wait_recv()
    y0.wait_recv()
    l_wo.wait()
    for c in (wx0, wy1, wx1, wy0):
        c.start()
    norm_rows(lat.at[1], 0, R, C + R)
    norm_rows(lat.at[2], 0, R, C + 2 * R)
    project_block(1, R)
    project_block(2, 2 * R)
    send_own(1)
    f0.wait_recv()
    f1.wait_recv()
    norm_rows(lat.at[3], 0, R, C + 3 * R)
    project_block(3, 3 * R)
    send_own(2)

    def arrive(dist, c):
        for direction in (0, 1):
            origin = s - dist if direction == 0 else s + dist
            here = origin >= 0 if direction == 0 else origin < n_sp

            @pl.when(here)
            def _():
                kv_copy(direction, dist, c, kvr.at[origin], origin, s).wait_recv()

            if dist + 2 < n_sp:
                side(direction, dist + 2, c, start)

    l_wq.wait()
    project_queries()
    q_copy = remote(qown.at[1 - e], qin, bs_q, br_q, {"sp": pair})
    q_copy.start()
    split_maps(qown[e], 0)
    arrive(1, 0)

    QB = 2 * R
    lift = lift_r[e]

    def attend(block, at, keys, start_row, count, first):
        k = block[at : at + keys, 0:HW]
        v = block[at : at + keys, HW:]
        vx = jnp.concatenate([v, jnp.ones_like(v)], axis=1)
        key = lax.broadcasted_iota(jnp.int32, (1, keys), 1)
        for m in range(2):
            for b in range(count // QB):
                rows = slice(start_row + b * QB, start_row + (b + 1) * QB)
                sc = lax.dot_general(
                    qm[m, rows, :], k, (((1,), (1,)), ((), ())), preferred_element_type=F32
                )
                if at < C:
                    sc = sc + jnp.where(key < C - at, lift, 0.0)
                p = jnp.exp(sc).astype(BF)
                add = jnp.dot(p, vx, preferred_element_type=F32)
                if first:
                    acc[m, rows, :] = add
                else:
                    acc[m, rows, :] += add

    def attend_arrived(dist, at, keys):
        @pl.when(s - dist >= 0)
        def _():
            attend(kvr.at[s - dist], at, keys, 0, 2 * ROWS, False)

        @pl.when(s + dist < n_sp)
        def _():
            attend(kvr.at[s + dist], at, keys, 0, 2 * ROWS, False)

    attend(kvl.at[e], 0, C + ROWS, 0, ROWS, True)
    for c in range(1, len(chunks)):
        arrive(1, c)
    wx0.wait_recv()
    wf0.start()
    wy1.wait_recv()
    wf1.start()
    q_copy.wait_recv()
    split_maps(qin[...], ROWS)
    attend(kvl.at[e], 0, C + ROWS, ROWS, ROWS, True)

    for dist in range(1, n_sp):
        last = dist == n_sp - 1
        if dist > 1:
            for c in range(len(chunks)):
                arrive(dist, c)
                if last:
                    attend_arrived(dist, *chunks[c])
        if not last:
            attend_arrived(dist, 0, C + ROWS)
        if dist == 2 or (last and n_sp == 2):
            wx1.wait_recv()
            dd_copy(1).start()
            wy0.wait_recv()
            dd_copy(2).start()

    def ho_copy(q, k):
        i = q * 4 + k
        where = {"tp": peers[k]} if q == 0 else {"sp": pair, "tp": peers[k]}
        if q == 1 and k == 0:
            where = {"sp": pair}
        return remote(mine.at[q, k], ho.at[q, k], bs_ho.at[i], br_ho.at[i], where)

    for q, k in ((1, 3), (1, 1), (1, 2), (0, 3), (1, 0), (0, 1), (0, 2), (0, 0)):
        rows = slice((4 * q + k) * R, (4 * q + k + 1) * R)
        a0 = acc[0, rows, :]
        a1 = acc[1, rows, :]
        mixed = a0[:, :VW] / a0[:, VW:] - lam_r[e] * (a1[:, :VW] / a1[:, VW:])
        inv = lax.rsqrt(jnp.mean(mixed * mixed, axis=-1, keepdims=True) + head_eps)
        mine[q, k, :, :] = (mixed * inv * v_gain * head_factor).astype(BF)
        if q or k:
            ho_copy(q, k).start()

    wf0.wait_recv()
    wf1.wait_recv()
    dd_copy(3).start()

    def head_rows(q):
        return pl.ds(pl.multiple_of((e if q == 0 else 1 - e) * VW, VW), VW)

    out = jnp.dot(mine[0, 0], wo[0, head_rows(0), :], preferred_element_type=F32)
    for q, k in ((0, 1), (0, 2), (1, 0), (0, 3), (1, 1), (1, 2), (1, 3)):
        if q == 0:
            dd_recv(k).wait_recv()
        ho_copy(q, k).wait_recv()
        out += jnp.dot(ho[q, k], wo[k, head_rows(q), :], preferred_element_type=F32)
    out_r[...] = vecs[4:5, :] * out

    for c in mod_copies + tp_copies + [x0, y1, x1, y0, f0, f1, wx0, wy1, wx1, wy0, wf0, wf1]:
        c.wait_send()
    for k in range(1, 4):
        dd_copy(k).wait_send()
    q_copy.wait_send()
    for q in range(2):
        for k in range(4):
            if q or k:
                ho_copy(q, k).wait_send()
    for dist in range(1, n_sp):
        for c in range(len(chunks)):
            for direction in (0, 1):
                side(direction, dist, c, drain)


def on_device(n_sp, n_tp, n_dp, *args):
    (
        latent, context, cond, context_cond, norm_gain, mod_shift, mod_scale, mod_gate,
        w_query, w_key, w_value, query_gain, key_gain, mix_lambda, context_lift, value_gain, w_out,
    ) = args
    R, D = latent.shape
    C = context.shape[0]
    head_width = query_gain.shape[0]
    cos, sin = rope_tables(R * n_sp * n_tp, head_width)
    QW, VWALL = w_query.shape[1], w_value.shape[1]
    heads = mix_lambda.shape[0]
    ROWS = R * n_tp
    MC = mod_shift.shape[1]
    chunk_sems = 2 * max(n_sp - 1, 1) * 3
    vm = pl.BlockSpec(memory_space=pltpu.VMEM)
    anywhere = pl.BlockSpec(memory_space=pl.ANY)
    smem = pl.BlockSpec(memory_space=pltpu.SMEM)
    dma = pltpu.SemaphoreType.DMA
    update = pl.pallas_call(
        functools.partial(kernel, n_sp, n_tp, n_dp, head_width),
        out_shape=pltpu.VMEM((R, D), F32),
        in_specs=[anywhere] * 14 + [smem, smem]
        + [anywhere] * 3,
        out_specs=vm,
        scratch_shapes=[
            pltpu.VMEM(cond.shape, BF),
            pltpu.VMEM(context_cond.shape, BF),
            pltpu.VMEM(norm_gain.shape, F32),
            pltpu.VMEM(query_gain.shape, F32),
            pltpu.VMEM(key_gain.shape, F32),
            pltpu.VMEM(value_gain.shape, F32),
            pltpu.VMEM((4, R, D), BF),
            pltpu.VMEM((C, D), BF),
            pltpu.VMEM((3,) + mod_shift.shape, BF),
            pltpu.VMEM(w_query.shape, BF),
            pltpu.VMEM(w_key.shape, BF),
            pltpu.VMEM(w_value.shape, BF),
            pltpu.VMEM((4,) + w_out.shape, BF),
            pltpu.VMEM((ROWS, 2 * head_width), F32),
            pltpu.VMEM((ROWS, 2 * head_width), F32),
            pltpu.VMEM((8, mod_shift.shape[0]), F32),
            pltpu.VMEM((8, MC), F32),
            pltpu.VMEM((max(n_sp - 1, 1), 8, MC), F32),
            pltpu.VMEM((8, MC), F32),
            pltpu.VMEM((n_tp, 8, MC), F32),
            pltpu.VMEM((8, D), F32),
            pltpu.VMEM((C + R, 128), F32),
            pltpu.VMEM((C + ROWS, D), BF),
            pltpu.VMEM((heads, ROWS, 2 * head_width), BF),
            pltpu.VMEM((ROWS, 2 * head_width), BF),
            pltpu.VMEM((2, 2 * ROWS, 2 * head_width), BF),
            pltpu.VMEM((heads, C + ROWS, (QW + VWALL) // heads), BF),
            pltpu.VMEM((n_sp, C + ROWS, (QW + VWALL) // heads), BF),
            pltpu.VMEM((2, 2 * ROWS, 2 * VWALL // heads), F32),
            pltpu.VMEM((2, 4, R, VWALL // heads), BF),
            pltpu.VMEM((2, 4, R, VWALL // heads), BF),
            dma((17,)),
            dma((6,)), dma((6,)),
            dma((max(n_sp - 1, 1),)), dma((max(n_sp - 1, 1),)),
            dma((3,)), dma((3,)),
            dma((chunk_sems,)), dma((chunk_sems,)),
            dma((6,)), dma((6,)),
            dma((3,)), dma((3,)),
            dma((8,)), dma((8,)),
            dma(()), dma(()),
        ],
        compiler_params=pltpu.CompilerParams(
            collective_id=0, has_side_effects=True, vmem_limit_bytes=66_100_000
        ),
        name="block",
    )(
        latent, context, cond, context_cond, norm_gain, mod_shift, mod_scale,
        mod_gate, w_query, w_key, w_value, query_gain, key_gain, value_gain, mix_lambda, context_lift, w_out,
        jnp.asarray(cos), jnp.asarray(sin),
    )
    return (latent.astype(F32) + update).astype(latent.dtype)


def solution(mesh):
    placed = (
        P(("dp", "sp", "tp"), None),
        P(("dp", "sp"), None),
        P(("dp", "sp")),
        P("sp"),
        P(),
        P("sp", "tp"),
        P("sp", "tp"),
        P("sp", "tp"),
        P(None, "tp"),
        P(None, "tp"),
        P(None, "tp"),
        P(),
        P(),
        P("tp"),
        P("tp"),
        P(),
        P("tp", None),
    )
    sizes = mesh.shape
    return jax.shard_map(
        functools.partial(on_device, sizes["sp"], sizes["tp"], sizes["dp"]),
        mesh=mesh,
        in_specs=placed,
        out_specs=P(("dp", "sp", "tp"), None),
        check_vma=False,
    )
```
